128 devices in a mesh: fs: 16 (over z, y), tp: 8 (over x, core).
Axes of the slice: x: 4, y: 4, z: 4, core: 2. Of those that a mesh axis runs over, the one named last changes fastest.
Arguments:
- late_input: bfloat16 [8192, 2048], P(('fs', 'tp')), may hold values from -6 to 6
- early_input: bfloat16 [8192, 2048], P(('fs', 'tp')), may hold values from -6 to 6
- early_grad: bfloat16 [8192, 2048], P(('fs', 'tp')), may hold values from -24 to 24
- pre_gain: float32 [2048], replicated, may hold values from 0.1 to 1.9
- post_gain: float32 [2048], replicated, may hold values from 0.1 to 1.9
- gate_weight: bfloat16 [2048, 4096], P('fs', 'tp'), may hold values from -0.125 to 0.125
- up_weight: bfloat16 [2048, 4096], P('fs', 'tp'), may hold values from -0.125 to 0.125
- down_weight: bfloat16 [2048, 4096], P('fs', 'tp'), may hold values from -0.09375 to 0.09375
- gate_sum: float32 [2048, 4096], P('fs', 'tp'), may hold values from -1.8 to 1.8
- up_sum: float32 [2048, 4096], P('fs', 'tp'), may hold values from -1.8 to 1.8
- down_gradient_sum: float32 [2048, 4096], P('fs', 'tp'), may hold values from -1.8 to 1.8
Outputs:
- late_output: bfloat16 [8192, 2048], P(('fs', 'tp'))
- early_input_grad: bfloat16 [8192, 2048], P(('fs', 'tp'))
- gate_total: float32 [2048, 4096], P('fs', 'tp')
- up_total: float32 [2048, 4096], P('fs', 'tp')
- down_total: float32 [2048, 4096], P('fs', 'tp')
The draws below stay inside these ranges and needn't reach their ends.
All inputs are finite; a program needn't handle non-finite values.
Results may differ from the reference program's by a relative error of at most 0.013.
Values may be sent and summed in bfloat16 or wider, within the bound.
A program may use at most 128 MiB of HBM per device.

```python
import math
import jax
import jax.numpy as jnp
from jax import lax

D = 2048
FF = 4096
ROWS = 8192
N_TP = 8


def with_spikes(array, rng, source, target, shards_of, factor):
    def block_of(position):
        return (jnp.arange(array.shape[position]) // (array.shape[position] // shards_of)).reshape((-1,) + (1,) * (array.ndim - 1 - position))

    one_side = jax.random.permutation(rng, shards_of)[block_of(target)]
    other_side = (block_of(target) + shards_of // 2) % shards_of
    return jnp.where((block_of(source) == one_side) | (block_of(source) == other_side), factor * array, array)


def shard_levels(own_key, shape, pieces, least, top_value):
    gain, own = 1.0, jax.random.fold_in(own_key, 6)
    for dim, shards_of in pieces:
        draws = jnp.exp(jax.random.uniform(jax.random.fold_in(own, dim), (shards_of,), jnp.float32, least / len(pieces), top_value / len(pieces)))
        gain = gain * jnp.repeat(draws, shape[dim] // shards_of).reshape([-1 if axis == dim else 1 for axis in range(len(shape))])
    return gain


def gaussian(rng, shape, scale, bound, split=(), held_as=jnp.bfloat16):
    loudness = shard_levels(rng, shape, split, -0.22, 0.18) if split else 1.0
    entries = jax.random.normal(rng, shape, jnp.float32) * scale * loudness
    return jnp.minimum(jnp.maximum(entries, -bound), bound).astype(held_as)


def noise_with(stream_key, shape, spread, limit, pieces, heavy, held_as=jnp.bfloat16):
    result = spread * jax.random.normal(stream_key, shape, jnp.float32)
    if pieces:
        result = result * shard_levels(stream_key, shape, pieces, -0.22, 0.18)
    return jnp.clip(with_spikes(result, jax.random.fold_in(stream_key, 3), *heavy), -limit, limit).astype(held_as)


def setup_inputs(seed: int = 0) -> dict:
    seeds = jax.random.split(jax.random.key(seed), 12)
    late_input = gaussian(seeds[0], (ROWS, D), 1.0, 6.0, ((0, 128),))
    early_input = gaussian(seeds[1], (ROWS, D), 1.0, 6.0, ((0, 128),))
    early_grad = noise_with(seeds[2], (ROWS, D), 1.0, 24.0, ((0, 128),), (0, 1, 128, 5.5))
    pre_gain = jnp.clip(1.0 + 0.18 * jax.random.normal(seeds[3], (D,), jnp.float32), 0.1, 1.9)
    post_gain = jnp.clip(1.0 + 0.18 * jax.random.normal(seeds[4], (D,), jnp.float32), 0.1, 1.9)
    gate_weight = gaussian(seeds[5], (D, FF), D ** -0.5, 0.125, ((0, 16), (1, 8)))
    up_weight = gaussian(seeds[6], (D, FF), D ** -0.5, 0.125, ((0, 16), (1, 8)))
    down_weight = gaussian(seeds[7], (D, FF), FF ** -0.5, 0.09375, ((0, 16), (1, 8)))
    gate_sum = gaussian(seeds[8], (D, FF), 0.3, 1.8, ((0, 16), (1, 8)), jnp.float32)
    up_sum = gaussian(seeds[9], (D, FF), 0.3, 1.8, ((0, 16), (1, 8)), jnp.float32)
    down_gradient_sum = gaussian(seeds[10], (D, FF), 0.3, 1.8, ((0, 16), (1, 8)), jnp.float32)
    return dict(late_input=late_input, early_input=early_input, early_grad=early_grad, pre_gain=pre_gain, post_gain=post_gain, gate_weight=gate_weight, up_weight=up_weight, down_weight=down_weight, gate_sum=gate_sum, up_sum=up_sum, down_gradient_sum=down_gradient_sum)


NORM_EPS = 1e-06

def contract_last(first_op, second_op):
    return lax.dot_general(first_op, second_op, (((1,), (1,)), ((), ())), preferred_element_type=jnp.float32)

def contract_first(first_op, second_op):
    return lax.dot_general(first_op, second_op, (((0,), (0,)), ((), ())), preferred_element_type=jnp.float32)

def inverse_rms(values):
    return lax.rsqrt(lax.optimization_barrier(jnp.mean(values * values, axis=-1, keepdims=True)) + NORM_EPS)

def rounded_blocks(term_of, row_count):
    running = jnp.zeros((row_count, D), jnp.float32)
    for block_index in range(N_TP):
        rounded = lax.optimization_barrier(term_of(block_index).astype(jnp.bfloat16))
        running = running + rounded.astype(jnp.float32)
    return running.astype(jnp.bfloat16)

def forward_rows(input_rows, pre_gain, gate_weight, up_weight, down_weight):
    values = input_rows.astype(jnp.float32)
    normed = (values * inverse_rms(values) * pre_gain).astype(jnp.bfloat16)
    gate_pre = jnp.dot(normed, gate_weight, preferred_element_type=jnp.float32)
    up_pre = jnp.dot(normed, up_weight, preferred_element_type=jnp.float32)
    hidden_state = (jax.nn.silu(gate_pre) * up_pre).astype(jnp.bfloat16)
    block_column_count = FF // N_TP

    def term_of(block_index):
        columns = slice(block_index * block_column_count, (block_index + 1) * block_column_count)
        return contract_last(hidden_state[:, columns], down_weight[:, columns])
    mixed = rounded_blocks(term_of, input_rows.shape[0])
    return (normed, gate_pre, up_pre, hidden_state, mixed)

def reference(late_input, early_input, early_grad, pre_gain, post_gain, gate_weight, up_weight, down_weight, gate_sum, up_sum, down_gradient_sum):
    late_mixed = forward_rows(late_input, pre_gain, gate_weight, up_weight, down_weight)[4]
    late_values = late_input.astype(jnp.float32)
    mixed_values = late_mixed.astype(jnp.float32)
    late_output = (late_values + 0.5 * mixed_values * inverse_rms(mixed_values) * post_gain).astype(jnp.bfloat16)
    normed, gate_pre, up_pre, hidden_state, mixed = forward_rows(early_input, pre_gain, gate_weight, up_weight, down_weight)
    early_mixed = mixed.astype(jnp.float32)
    inverse_norm = inverse_rms(early_mixed)
    weighted = 0.5 * early_grad.astype(jnp.float32) * post_gain
    mixed_cot = (inverse_norm * weighted - early_mixed * inverse_norm ** 3 * lax.optimization_barrier(jnp.mean(weighted * early_mixed, axis=-1, keepdims=True))).astype(jnp.bfloat16)
    hidden_cot = jnp.dot(mixed_cot, down_weight, preferred_element_type=jnp.float32)
    sigmoid_gate = jax.nn.sigmoid(gate_pre)
    gate_cot = (hidden_cot * up_pre * sigmoid_gate * (1.0 + gate_pre * (1.0 - sigmoid_gate))).astype(jnp.bfloat16)
    up_cot = (hidden_cot * gate_pre * sigmoid_gate).astype(jnp.bfloat16)
    block_column_count = FF // N_TP

    def back_term(block_index):
        columns = slice(block_index * block_column_count, (block_index + 1) * block_column_count)
        return contract_last(gate_cot[:, columns], gate_weight[:, columns]) + contract_last(up_cot[:, columns], up_weight[:, columns])
    normed_cot = rounded_blocks(back_term, early_input.shape[0]).astype(jnp.float32)
    early_values = early_input.astype(jnp.float32)
    early_inverse_norm = inverse_rms(early_values)
    weighted_in = normed_cot * pre_gain
    early_input_grad = (early_grad.astype(jnp.float32) + early_inverse_norm * weighted_in - early_values * early_inverse_norm ** 3 * lax.optimization_barrier(jnp.mean(weighted_in * early_values, axis=-1, keepdims=True))).astype(jnp.bfloat16)
    grad_scale = 1.0 / math.sqrt(ROWS)
    gate_total = gate_sum + grad_scale * contract_first(normed, gate_cot)
    up_total = up_sum + grad_scale * contract_first(normed, up_cot)
    down_total = down_gradient_sum + grad_scale * contract_first(mixed_cot, hidden_state)
    return (late_output, early_input_grad, gate_total, up_total, down_total)
```

```python
import math

import jax
import jax.numpy as jnp
from jax import lax
from jax.experimental import pallas as pl
from jax.experimental.pallas import tpu as pltpu
from jax.sharding import PartitionSpec as P

NORM_EPS = 1e-06
BF = jnp.bfloat16
F32 = jnp.float32
MESH = pl.DeviceIdType.MESH

ORDER = [
    (0, 0), (0, 1), (0, -1), (1, 0),
    (-1, 0), (2, 0), (1, 1), (1, -1),
    (-1, 1), (-1, -1), (0, 2), (1, 2),
    (-1, 2), (2, 1), (2, -1), (2, 2),
]
HOPS = (
    [((0, 0), ax, sg, None) for ax in "ab" for sg in (1, -1)]
    + [((2, 0), "b", sg, None) for sg in (1, -1)]
    + [((0, s), "a", sg, None) for s in (1, -1) for sg in (1, -1)]
    + [((0, s), "b", -s, (1 + s) // 2) for s in (1, -1)]
    + [((s, t), "b", -t, (1 + t) // 2) for s in (1, -1) for t in (1, -1)]
    + [((s, 0), "a", -s, (1 + s) // 2) for s in (1, -1)]
    + [((s, 2), "a", -s, (1 + s) // 2) for s in (1, -1)]
)


def wrapped(n):
    n %= 4
    return n - 4 if n == 3 else n


def landing(hop):
    (da, db), ax, sg, _ = hop
    if ax == "a":
        da -= sg
    else:
        db -= sg
    return (wrapped(db), wrapped(da))


LANDS = [ORDER.index(landing(hop)) for hop in HOPS]
ARRIVALS = {o: [i for i, k in enumerate(LANDS) if ORDER[k] == o] for o in ORDER}
DUTIES = {o: [i for i, hop in enumerate(HOPS) if hop[0] == o] for o in ORDER}
SLOT, _at = [], 0
for _hop in HOPS:
    SLOT.append(_at)
    _at += 128 if _hop[3] is None else 64
ARRIVED_ROWS = _at


def rows_of(k, part):
    return (k * 128, 128) if part is None else (k * 128 + 64 * part, 64)


def last_last(a, b):
    return lax.dot_general(a, b, (((1,), (1,)), ((), ())), preferred_element_type=F32)


def first_first(a, b):
    return lax.dot_general(a, b, (((0,), (0,)), ((), ())), preferred_element_type=F32)


def kernel(
    late_in, early_in, early_grad, pre_gain, post_gain, gate_w, up_w, down_w,
    gate_sum, up_sum, down_sum,
    late_out, early_out, gate_out, up_out, down_out,
    w_all, tok, tok_t, pre, dgate, dup, hid, part, pair, both, fwd, last, cot, hcot,
    gcot, ucot, grads, arrived, mixed, weighted,
    ag_s, ag_r, rs_s, rs_r, xa_s, xa_r, xr_s, xr_r,
):
    fs = lax.axis_index("fs")
    tp = lax.axis_index("tp")
    y, z = fs % 4, fs // 4
    par = (y + z) % 2
    core, x = tp % 2, tp // 2
    grad_scale = 1.0 / math.sqrt(8192.0)

    def fs_at(da, db):
        dy = (1 - par) * da + par * db
        dz = (1 - par) * db + par * da
        return ((z + dz + 4) % 4) * 4 + (y + dy + 4) % 4

    def torus(ax, sg):
        return (fs_at(sg, 0) if ax == "a" else fs_at(0, sg), tp)

    ring = {sg: (fs, ((x + sg + 4) % 4) * 2 + core) for sg in (1, -1)}
    partner = (fs, x * 2 + 1 - core)
    columns = [pl.multiple_of(fs_at(*o) * 128, 128) for o in ORDER]

    barrier = pltpu.get_barrier_semaphore()
    peers = [partner, ring[1], ring[-1]] + [torus(ax, sg) for ax in "ab" for sg in (1, -1)]
    for peer in peers:
        pl.semaphore_signal(barrier, inc=1, device_id=peer, device_id_type=MESH)
    pl.semaphore_wait(barrier, len(peers))

    sent = []

    def send(src, dst, ss, rs, to):
        copy = pltpu.make_async_remote_copy(
            src_ref=src, dst_ref=dst, send_sem=ss, recv_sem=rs,
            device_id=to, device_id_type=MESH,
        )
        copy.start()
        sent.append(copy)

    def arrive(dst, ss, rs):
        pltpu.make_async_remote_copy(
            src_ref=dst, dst_ref=dst, send_sem=ss, recv_sem=rs,
            device_id=partner, device_id_type=MESH,
        ).wait_recv()

    own_w = (gate_w, up_w, down_w)

    def pass_on(w, offset):
        for i in DUTIES[offset]:
            _, ax, sg, q = HOPS[i]
            start, n = rows_of(ORDER.index(offset), q)
            src = own_w[w] if offset == (0, 0) else w_all.at[w, pl.ds(start, n)]
            there, _ = rows_of(LANDS[i], q)
            send(src, w_all.at[w, pl.ds(there, n)], ag_s.at[w, i], ag_r.at[w, i], torus(ax, sg))

    def take(w, offset):
        for i in ARRIVALS[offset]:
            start, n = rows_of(LANDS[i], HOPS[i][3])
            arrive(w_all.at[w, pl.ds(start, n)], ag_s.at[w, i], ag_r.at[w, i])

    def relay(w, offsets):
        for offset in offsets:
            take(w, offset)
            pass_on(w, offset)

    near = [(0, 1), (0, -1), (1, 0), (-1, 0)]
    mid = [(2, 0), (1, 1), (1, -1), (-1, 1), (-1, -1), (0, 2)]
    far = [(1, 2), (-1, 2), (2, 1), (2, -1)]
    end = [(2, 2)]

    def spread(j, view):
        send(view(0, 64), view(192, 64), xa_s.at[j, 0], xa_r.at[j, 0], ring[1])
        send(view(0, 64), view(64, 64), xa_s.at[j, 1], xa_r.at[j, 1], ring[-1])
        send(view(0, 64), view(256, 64), xa_s.at[j, 4], xa_r.at[j, 4], partner)

    def spread_near(j, view):
        arrive(view(192, 64), xa_s.at[j, 0], xa_r.at[j, 0])
        send(view(192, 32), view(128, 32), xa_s.at[j, 2], xa_r.at[j, 2], ring[1])
        send(view(192, 64), view(448, 64), xa_s.at[j, 7], xa_r.at[j, 7], partner)
        arrive(view(64, 64), xa_s.at[j, 1], xa_r.at[j, 1])
        send(view(96, 32), view(160, 32), xa_s.at[j, 3], xa_r.at[j, 3], ring[-1])
        send(view(64, 64), view(320, 64), xa_s.at[j, 5], xa_r.at[j, 5], partner)

    def spread_far(j, view):
        arrive(view(128, 32), xa_s.at[j, 2], xa_r.at[j, 2])
        arrive(view(160, 32), xa_s.at[j, 3], xa_r.at[j, 3])
        send(view(128, 64), view(384, 64), xa_s.at[j, 6], xa_r.at[j, 6], partner)

    def spread_end(j, view):
        for i, row in ((4, 256), (5, 320), (7, 448), (6, 384)):
            arrive(view(row, 64), xa_s.at[j, i], xa_r.at[j, i])

    def tok_view(m):
        return lambda row, n: tok.at[m, pl.ds(row, n)]

    def cot_view(g):
        return lambda row, n: cot.at[pl.ds(row, n), pl.ds(512 * g, 512)]

    def sum_pair(v, g):
        s = 4 * v + g
        send(part.at[v, g, pl.ds(256, 256)], pair.at[v, g], xr_s.at[s, 0], xr_r.at[s, 0], partner)

    def sum_start(v, g):
        s = 4 * v + g
        arrive(pair.at[v, g], xr_s.at[s, 0], xr_r.at[s, 0])
        both[v, g] = (part[v, g, :256].astype(F32) + pair[v, g].astype(F32)).astype(BF)
        send(
            both.at[v, g, pl.ds(128, 32)], fwd.at[v, g, pl.ds(0, 32)],
            xr_s.at[s, 1], xr_r.at[s, 1], ring[1],
        )
        send(
            both.at[v, g, pl.ds(160, 32)], fwd.at[v, g, pl.ds(32, 32)],
            xr_s.at[s, 2], xr_r.at[s, 2], ring[-1],
        )

    def sum_middle(v, g):
        s = 4 * v + g
        arrive(fwd.at[v, g, pl.ds(0, 32)], xr_s.at[s, 1], xr_r.at[s, 1])
        both[v, g, 64:96] = (both[v, g, 64:96].astype(F32) + fwd[v, g, :32].astype(F32)).astype(BF)
        send(
            both.at[v, g, pl.ds(64, 64)], last.at[v, g, pl.ds(0, 64)],
            xr_s.at[s, 3], xr_r.at[s, 3], ring[1],
        )
        arrive(fwd.at[v, g, pl.ds(32, 32)], xr_s.at[s, 2], xr_r.at[s, 2])
        both[v, g, 224:256] = (
            both[v, g, 224:256].astype(F32) + fwd[v, g, 32:].astype(F32)
        ).astype(BF)
        send(
            both.at[v, g, pl.ds(192, 64)], last.at[v, g, pl.ds(64, 64)],
            xr_s.at[s, 4], xr_r.at[s, 4], ring[-1],
        )

    def sum_end(v, g):
        s = 4 * v + g
        arrive(last.at[v, g, pl.ds(0, 64)], xr_s.at[s, 3], xr_r.at[s, 3])
        arrive(last.at[v, g, pl.ds(64, 64)], xr_s.at[s, 4], xr_r.at[s, 4])
        total = both[v, g, :64].astype(F32) + last[v, g, :64].astype(F32)
        mixed[v, :, pl.ds(512 * g, 512)] = (total + last[v, g, 64:].astype(F32)).astype(BF)

    def give(w, offset):
        k = ORDER.index(offset)
        for i in ARRIVALS[offset]:
            _, ax, sg, q = HOPS[i]
            start, n = rows_of(k, q)
            send(
                grads.at[w, pl.ds(start, n)], arrived.at[w, pl.ds(SLOT[i], n)],
                rs_s.at[w, i], rs_r.at[w, i], torus("b" if ax == "a" else "a", -sg),
            )

    def gain(w, offset):
        k = ORDER.index(offset)
        for i in DUTIES[offset]:
            start, n = rows_of(k, HOPS[i][3])
            arrive(arrived.at[w, pl.ds(SLOT[i], n)], rs_s.at[w, i], rs_r.at[w, i])
        halves = [i for i in DUTIES[offset] if HOPS[i][3] is not None]
        wholes = [i for i in DUTIES[offset] if HOPS[i][3] is None]
        for q in (0, 1):
            terms = [SLOT[i] + 64 * q for i in wholes]
            terms += [SLOT[i] for i in halves if HOPS[i][3] == q]
            if terms:
                start, _ = rows_of(k, q)
                total = grads[w, start : start + 64].astype(F32)
                for at in terms:
                    total += arrived[w, at : at + 64].astype(F32)
                grads[w, start : start + 64] = total.astype(BF)

    def combine(w, offsets):
        for offset in offsets:
            gain(w, offset)
            give(w, offset)

    def finish(w, old, out):
        for i in DUTIES[(0, 0)]:
            arrive(arrived.at[w, pl.ds(SLOT[i], 128)], rs_s.at[w, i], rs_r.at[w, i])
        for q in (0, 1):
            total = grads[w, 64 * q : 64 * q + 64].astype(F32)
            for i in DUTIES[(0, 0)]:
                at = SLOT[i] + 64 * q
                total += arrived[w, at : at + 64].astype(F32)
            out[64 * q : 64 * q + 64] = old[64 * q : 64 * q + 64] + grad_scale * total

    def tiles(count, body):
        lax.fori_loop(0, count, lambda i, c: (body(i), c)[1], 0)

    def norm_tokens(m, source):
        values = source[...].astype(F32)
        inverse = lax.rsqrt(jnp.mean(values * values, axis=-1, keepdims=True) + NORM_EPS)
        for k, at in enumerate(columns):
            tok[m, 0:64, 128 * k : 128 * k + 128] = (
                source[:, pl.ds(at, 128)].astype(F32) * inverse * pre_gain[:, pl.ds(at, 128)]
            ).astype(BF)

    def gate_product(m):
        def body(i):
            r = pl.multiple_of(i * 128, 128)
            pre[m, pl.ds(r, 128)] = jnp.dot(
                tok[m, pl.ds(r, 128)], w_all[0], preferred_element_type=F32
            )

        tiles(4, body)

    def up_product(m):
        def body(i):
            r = pl.multiple_of(i * 128, 128)
            up = jnp.dot(tok[m, pl.ds(r, 128)], w_all[1], preferred_element_type=F32)
            gate = pre[m, pl.ds(r, 128)]
            s = jax.nn.sigmoid(gate)
            hid[m, pl.ds(r, 128)] = (gate * s * up).astype(BF)
            if m == 1:
                dgate[pl.ds(r, 128)] = up * s * (1.0 + gate * (1.0 - s))
                dup[pl.ds(r, 128)] = gate * s

        tiles(4, body)

    def down_product(m, v, g):
        def body(i):
            r = pl.multiple_of(i * 256, 256)
            part[v, g, pl.ds(r, 256)] = last_last(
                hid[m, pl.ds(r, 256)], w_all[2, pl.ds(512 * g, 512)]
            ).astype(BF)

        tiles(2, body)

    def back_product(g):
        def body(i):
            r = pl.multiple_of(i * 256, 256)
            part[2, g, pl.ds(r, 256)] = (
                last_last(gcot[pl.ds(r, 256)], w_all[0, pl.ds(512 * g, 512)])
                + last_last(ucot[pl.ds(r, 256)], w_all[1, pl.ds(512 * g, 512)])
            ).astype(BF)

        tiles(2, body)

    def hidden_product(g, first):
        def body(i):
            r = pl.multiple_of(i * 256, 256)
            term = jnp.dot(
                cot[pl.ds(r, 256), pl.ds(512 * g, 512)],
                w_all[2, pl.ds(512 * g, 512)],
                preferred_element_type=F32,
            )
            hcot[pl.ds(r, 256)] = term if first else hcot[pl.ds(r, 256)] + term

        tiles(2, body)

    def down_gradient(g):
        grads[2, pl.ds(512 * g, 512)] = first_first(
            cot[:, pl.ds(512 * g, 512)], hid[1]
        ).astype(BF)

    def turn_tokens():
        for k in range(16):
            tok_t[128 * k : 128 * k + 128] = tok[1, :, 128 * k : 128 * k + 128].T

    def weight_gradient(w, g, values):
        def body(i):
            r = pl.multiple_of(512 * g + i * 256, 256)
            grads[w, pl.ds(r, 256)] = jnp.dot(
                tok_t[pl.ds(r, 256)], values[...], preferred_element_type=F32
            ).astype(BF)

        tiles(2, body)

    pass_on(0, (0, 0))
    norm_tokens(1, early_in)
    spread(1, tok_view(1))
    pass_on(1, (0, 0))
    norm_tokens(0, late_in)
    spread(0, tok_view(0))
    for w in range(3):
        w_all[w, 0:128] = own_w[w][...]
    for k, at in enumerate(columns):
        weighted[:, 128 * k : 128 * k + 128] = (
            0.5 * early_grad[:, pl.ds(at, 128)].astype(F32) * post_gain[:, pl.ds(at, 128)]
        )
    relay(0, near)
    spread_near(1, tok_view(1))
    relay(1, near)
    pass_on(2, (0, 0))
    relay(0, mid)
    spread_far(1, tok_view(1))
    relay(0, far)
    relay(2, near)
    relay(1, mid)
    spread_near(0, tok_view(0))
    relay(0, end)
    spread_end(1, tok_view(1))
    gate_product(1)
    relay(1, far)
    spread_far(0, tok_view(0))
    relay(2, mid)
    turn_tokens()
    relay(1, end)
    up_product(1)
    down_product(1, 0, 0)
    sum_pair(0, 0)
    down_product(1, 0, 1)
    sum_pair(0, 1)
    relay(2, far)
    sum_start(0, 0)
    down_product(1, 0, 2)
    sum_pair(0, 2)
    sum_start(0, 1)
    spread_end(0, tok_view(0))
    gate_product(0)
    sum_middle(0, 0)
    sum_start(0, 2)
    sum_middle(0, 1)
    relay(2, end)
    down_product(1, 0, 3)
    sum_pair(0, 3)
    sum_middle(0, 2)
    sum_end(0, 0)
    sum_start(0, 3)
    sum_end(0, 1)
    up_product(0)
    sum_middle(0, 3)
    sum_end(0, 2)
    down_product(0, 1, 0)
    sum_pair(1, 0)
    sum_end(0, 3)

    values = mixed[0].astype(F32)
    inverse = lax.rsqrt(jnp.mean(values * values, axis=-1, keepdims=True) + NORM_EPS)
    scaled = inverse**3 * jnp.mean(weighted[...] * values, axis=-1, keepdims=True)
    cot[0:64] = (inverse * weighted[...] - values * scaled).astype(BF)
    for g in (3, 2, 1, 0):
        spread(g + 2, cot_view(g))
    for g in (1, 2, 3):
        down_product(0, 1, g)
        sum_pair(1, g)
    for g in (3, 2, 1, 0):
        spread_near(g + 2, cot_view(g))
        spread_far(g + 2, cot_view(g))
        spread_end(g + 2, cot_view(g))
        down_gradient(g)
        if g == 3:
            for o in end + [(2, 1), (2, -1)]:
                give(2, o)
        if g == 2:
            give(2, (0, 2))
        hidden_product(g, g == 3)
        sum_start(1, g)
    combine(2, [(1, 2), (-1, 2)])

    gcot[...] = (hcot[...] * dgate[...]).astype(BF)
    ucot[...] = (hcot[...] * dup[...]).astype(BF)
    for w, values_of in ((0, gcot), (1, ucot)):
        weight_gradient(w, 3, values_of)
        for o in end + [(2, 1), (2, -1)]:
            give(w, o)
        weight_gradient(w, 2, values_of)
        give(w, (0, 2))
        if w == 0:
            combine(2, [(1, 1), (1, -1), (-1, 1), (-1, -1)])
        weight_gradient(w, 1, values_of)
        weight_gradient(w, 0, values_of)
        if w == 0:
            combine(2, [(2, 0), (1, 0), (-1, 0)])
            combine(0, [(1, 2), (-1, 2)])
    for g in range(4):
        back_product(g)
        sum_pair(2, g)
    for g in (3, 2, 1, 0):
        sum_middle(1, g)
    combine(0, [(1, 1), (1, -1), (-1, 1), (-1, -1)])
    combine(1, [(1, 2), (-1, 2)])
    combine(2, [(0, 1), (0, -1)])
    combine(0, [(2, 0), (1, 0), (-1, 0)])
    for g in range(4):
        sum_end(1, g)
        sum_start(2, g)
    combine(1, [(1, 1), (1, -1), (-1, 1), (-1, -1)])

    late_mixed = mixed[1].astype(F32)
    late_inverse = lax.rsqrt(jnp.mean(late_mixed * late_mixed, axis=-1, keepdims=True) + NORM_EPS)
    for k, at in enumerate(columns):
        late_out[:, pl.ds(at, 128)] = (
            late_in[:, pl.ds(at, 128)].astype(F32)
            + 0.5
            * mixed[1, :, 128 * k : 128 * k + 128].astype(F32)
            * late_inverse
            * post_gain[:, pl.ds(at, 128)]
        ).astype(BF)

    combine(0, [(0, 1), (0, -1)])
    combine(1, [(2, 0), (1, 0), (-1, 0)])
    for g in range(4):
        sum_middle(2, g)
    finish(2, down_sum, down_out)
    combine(1, [(0, 1), (0, -1)])
    for g in range(4):
        sum_end(2, g)

    early = early_in[...].astype(F32)
    early_inverse = lax.rsqrt(jnp.mean(early * early, axis=-1, keepdims=True) + NORM_EPS)
    dots = jnp.zeros((64, 128), F32)
    for k, at in enumerate(columns):
        dots += (
            mixed[2, :, 128 * k : 128 * k + 128].astype(F32)
            * pre_gain[:, pl.ds(at, 128)]
            * early_in[:, pl.ds(at, 128)].astype(F32)
        )
    slope = early_inverse**3 * (jnp.sum(dots, axis=-1, keepdims=True) * (1.0 / 2048.0))
    for k, at in enumerate(columns):
        early_out[:, pl.ds(at, 128)] = (
            early_grad[:, pl.ds(at, 128)].astype(F32)
            + early_inverse
            * (mixed[2, :, 128 * k : 128 * k + 128].astype(F32) * pre_gain[:, pl.ds(at, 128)])
            - early_in[:, pl.ds(at, 128)].astype(F32) * slope
        ).astype(BF)

    finish(0, gate_sum, gate_out)
    finish(1, up_sum, up_out)
    for copy in sent:
        copy.wait_send()


def per_device(
    late_input,
    early_input,
    early_grad,
    pre_gain,
    post_gain,
    gate_weight,
    up_weight,
    down_weight,
    gate_sum,
    up_sum,
    down_gradient_sum,
):
    sem = pltpu.SemaphoreType.DMA
    vmem = pltpu.VMEM
    tokens = jax.ShapeDtypeStruct((64, 2048), BF)
    total = jax.ShapeDtypeStruct((128, 512), F32)
    return pl.pallas_call(
        kernel,
        name="half_step",
        out_shape=(tokens, tokens, total, total, total),
        in_specs=[pl.BlockSpec(memory_space=vmem)] * 11,
        out_specs=[pl.BlockSpec(memory_space=vmem)] * 5,
        scratch_shapes=[
            vmem((3, 2048, 512), BF),
            vmem((2, 512, 2048), BF),
            vmem((2048, 512), BF),
            vmem((2, 512, 512), F32),
            vmem((512, 512), F32),
            vmem((512, 512), F32),
            vmem((2, 512, 512), BF),
            vmem((3, 4, 512, 512), BF),
            vmem((3, 4, 256, 512), BF),
            vmem((3, 4, 256, 512), BF),
            vmem((3, 4, 64, 512), BF),
            vmem((3, 4, 128, 512), BF),
            vmem((512, 2048), BF),
            vmem((512, 512), F32),
            vmem((512, 512), BF),
            vmem((512, 512), BF),
            vmem((3, 2048, 512), BF),
            vmem((3, ARRIVED_ROWS, 512), BF),
            vmem((3, 64, 2048), BF),
            vmem((64, 2048), F32),
            sem((3, 20)),
            sem((3, 20)),
            sem((3, 20)),
            sem((3, 20)),
            sem((6, 8)),
            sem((6, 8)),
            sem((12, 5)),
            sem((12, 5)),
        ],
        compiler_params=pltpu.CompilerParams(
            collective_id=0, has_side_effects=True, vmem_limit_bytes=67043328
        ),
    )(
        late_input, early_input, early_grad, pre_gain.reshape(1, -1), post_gain.reshape(1, -1),
        gate_weight, up_weight, down_weight, gate_sum, up_sum, down_gradient_sum,
    )


def solution(mesh):
    rows, both = P(("fs", "tp"), None), P("fs", "tp")
    return jax.shard_map(
        per_device,
        mesh=mesh,
        in_specs=(rows,) * 3 + (P(), P()) + (both,) * 6,
        out_specs=(rows, rows, both, both, both),
        check_vma=False,
    )
```

```python
import math

import jax
import jax.numpy as jnp
from jax import lax
from jax.experimental import pallas as pl
from jax.experimental.pallas import tpu as pltpu
from jax.sharding import PartitionSpec as P

NORM_EPS = 1e-06
BF = jnp.bfloat16
F32 = jnp.float32
MESH = pl.DeviceIdType.MESH

ORDER = [
    (0, 0), (0, 1), (0, -1), (1, 0),
    (-1, 0), (2, 0), (1, 1), (1, -1),
    (-1, 1), (-1, -1), (0, 2), (1, 2),
    (-1, 2), (2, 1), (2, -1), (2, 2),
]
HOPS = (
    [((0, 0), ax, sg, None) for ax in "ab" for sg in (1, -1)]
    + [((2, 0), "b", sg, None) for sg in (1, -1)]
    + [((0, s), "a", sg, None) for s in (1, -1) for sg in (1, -1)]
    + [((0, s), "b", -s, (1 + s) // 2) for s in (1, -1)]
    + [((s, t), "b", -t, (1 + t) // 2) for s in (1, -1) for t in (1, -1)]
    + [((s, 0), "a", -s, (1 + s) // 2) for s in (1, -1)]
    + [((s, 2), "a", -s, (1 + s) // 2) for s in (1, -1)]
)


(
    OWN, RELAY, NORM, SPREAD, NEAR, FAR, FULL, WEIGH, GATE, UP, DOWN, BACK, START, MIDDLE,
    SUMMED, TURN, COT, HIDDEN, DGRAD, DERIVE, WGRAD, COMBINE, LATE, EARLY,
) = range(24)
SCRIPT = [
    (NORM, 1), (SPREAD, 1), (OWN, 0), (NORM, 0), (OWN, 1), (SPREAD, 0), (OWN, 2), (OWN, 3),
    (WEIGH,), (RELAY, 0, 1), (RELAY, 0, 3), (RELAY, 0, 4), (RELAY, 0, 2), (RELAY, 1, 1),
    (RELAY, 1, 3), (RELAY, 1, 4), (RELAY, 1, 2), (RELAY, 2, 1), (RELAY, 2, 3), (RELAY, 2, 4),
    (RELAY, 2, 2), (NEAR, 1, -1), (NEAR, 1, 1), (RELAY, 3, 1), (RELAY, 3, 3), (RELAY, 3, 4),
    (RELAY, 3, 2), (RELAY, 0, 5), (RELAY, 0, 6), (RELAY, 0, 7), (RELAY, 1, 6), (RELAY, 0, 10),
    (RELAY, 1, 7), (RELAY, 1, 10), (RELAY, 0, 8), (RELAY, 0, 9), (RELAY, 1, 8), (RELAY, 1, 5),
    (RELAY, 1, 9), (RELAY, 2, 5), (NEAR, 0, -1), (NEAR, 0, 1), (RELAY, 2, 6), (RELAY, 2, 7),
    (RELAY, 3, 6), (RELAY, 2, 10), (RELAY, 3, 7), (RELAY, 3, 10), (RELAY, 2, 8), (RELAY, 2, 9),
    (OWN, 4), (FAR, 1), (RELAY, 3, 5), (RELAY, 3, 8), (RELAY, 3, 9), (OWN, 5), (RELAY, 1, 13),
    (RELAY, 0, 11), (RELAY, 0, 12), (FULL, 1), (TURN,), (RELAY, 0, 13), (RELAY, 1, 12), (FAR, 0),
    (RELAY, 0, 14), (RELAY, 1, 11), (RELAY, 1, 14), (RELAY, 3, 13), (RELAY, 2, 11),
    (RELAY, 2, 12), (FULL, 0), (RELAY, 2, 13), (RELAY, 4, 1), (RELAY, 4, 2), (RELAY, 2, 14),
    (RELAY, 3, 11), (RELAY, 3, 12), (RELAY, 3, 14), (RELAY, 4, 3), (RELAY, 4, 4), (RELAY, 5, 1),
    (RELAY, 5, 3), (RELAY, 5, 4), (RELAY, 5, 2), (RELAY, 0, 15), (RELAY, 1, 15), (GATE, 1, 0),
    (GATE, 1, 1), (RELAY, 2, 15), (RELAY, 4, 5), (GATE, 1, 2), (RELAY, 3, 15), (GATE, 1, 3),
    (UP, 1, 0), (RELAY, 4, 6), (RELAY, 4, 7), (UP, 1, 1), (UP, 1, 2), (RELAY, 5, 6),
    (RELAY, 5, 7), (UP, 1, 3), (RELAY, 4, 8), (RELAY, 4, 9), (DOWN, 0, 0), (RELAY, 4, 10),
    (RELAY, 5, 10), (GATE, 0, 0), (RELAY, 5, 5), (GATE, 0, 1), (RELAY, 5, 8), (DOWN, 0, 1),
    (RELAY, 5, 9), (GATE, 0, 2), (START, 0, 0), (RELAY, 4, 11), (RELAY, 4, 12), (RELAY, 5, 13),
    (DOWN, 0, 2), (RELAY, 4, 13), (GATE, 0, 3), (START, 0, 1), (UP, 0, 0), (RELAY, 4, 14),
    (UP, 0, 1), (RELAY, 5, 11), (RELAY, 5, 12), (UP, 0, 2), (START, 0, 2), (UP, 0, 3),
    (MIDDLE, 0, 0, -1), (MIDDLE, 0, 0, 1), (RELAY, 5, 14), (DOWN, 1, 0), (RELAY, 4, 15),
    (DOWN, 1, 1), (MIDDLE, 0, 1, -1), (MIDDLE, 0, 1, 1), (DOWN, 1, 2), (RELAY, 5, 15),
    (DOWN, 0, 3), (MIDDLE, 0, 2, -1), (MIDDLE, 0, 2, 1), (DOWN, 1, 3), (SUMMED, 0, 0),
    (START, 0, 3), (SUMMED, 0, 1), (SUMMED, 0, 2), (SUMMED, 0, 3), (COT,), (SPREAD, 5),
    (SPREAD, 4), (SPREAD, 3), (SPREAD, 2), (NEAR, 5, -1), (FAR, 5), (NEAR, 4, -1), (NEAR, 5, 1),
    (NEAR, 3, -1), (FULL, 5), (DGRAD, 3), (NEAR, 4, 1), (NEAR, 2, -1), (COMBINE, 4, 15),
    (COMBINE, 5, 15), (COMBINE, 4, 13), (COMBINE, 4, 14), (COMBINE, 5, 14), (HIDDEN, 3),
    (NEAR, 3, 1), (START, 1, 0), (START, 1, 1), (START, 1, 2), (START, 1, 3), (NEAR, 2, 1),
    (FAR, 4), (COMBINE, 4, 12), (COMBINE, 5, 11), (COMBINE, 5, 12), (FAR, 3), (MIDDLE, 1, 0, -1),
    (FULL, 4), (DGRAD, 2), (COMBINE, 5, 13), (COMBINE, 4, 10), (COMBINE, 4, 11), (COMBINE, 4, 8),
    (COMBINE, 4, 9), (COMBINE, 5, 9), (HIDDEN, 2), (FULL, 3), (DGRAD, 1), (COMBINE, 5, 10),
    (COMBINE, 4, 6), (COMBINE, 4, 7), (COMBINE, 5, 8), (HIDDEN, 1), (MIDDLE, 1, 0, 1),
    (MIDDLE, 1, 1, -1), (MIDDLE, 1, 1, 1), (MIDDLE, 1, 2, -1), (MIDDLE, 1, 2, 1),
    (MIDDLE, 1, 3, -1), (MIDDLE, 1, 3, 1), (COMBINE, 5, 5), (FAR, 2), (COMBINE, 5, 6),
    (COMBINE, 5, 7), (COMBINE, 4, 4), (COMBINE, 4, 5), (FULL, 2), (DGRAD, 0), (COMBINE, 4, 3),
    (HIDDEN, 0), (DERIVE,), (COMBINE, 5, 3), (COMBINE, 5, 4), (WGRAD, 0, 3), (COMBINE, 0, 15),
    (COMBINE, 1, 15), (COMBINE, 0, 13), (COMBINE, 0, 14), (COMBINE, 1, 14), (WGRAD, 0, 2),
    (COMBINE, 1, 13), (COMBINE, 0, 10), (WGRAD, 0, 1), (COMBINE, 1, 10), (WGRAD, 0, 0),
    (COMBINE, 5, 1), (COMBINE, 5, 2), (WGRAD, 1, 3), (COMBINE, 4, 1), (COMBINE, 2, 15),
    (COMBINE, 3, 15), (COMBINE, 2, 13), (COMBINE, 2, 14), (COMBINE, 3, 14), (WGRAD, 1, 2),
    (COMBINE, 4, 2), (COMBINE, 3, 13), (COMBINE, 2, 10), (WGRAD, 1, 1), (COMBINE, 0, 11),
    (COMBINE, 0, 12), (COMBINE, 1, 12), (COMBINE, 3, 10), (WGRAD, 1, 0), (COMBINE, 1, 11),
    (COMBINE, 0, 7), (COMBINE, 1, 8), (COMBINE, 1, 9), (SUMMED, 1, 0), (SUMMED, 1, 1),
    (SUMMED, 1, 2), (SUMMED, 1, 3), (BACK, 0), (COMBINE, 0, 6), (COMBINE, 0, 8), (COMBINE, 0, 9),
    (COMBINE, 1, 6), (COMBINE, 1, 7), (BACK, 1), (COMBINE, 2, 12), (COMBINE, 0, 3),
    (COMBINE, 0, 4), (COMBINE, 1, 3), (COMBINE, 1, 4), (BACK, 2), (COMBINE, 5, 0),
    (COMBINE, 3, 9), (START, 2, 0), (BACK, 3), (COMBINE, 2, 11), (COMBINE, 3, 11),
    (COMBINE, 3, 12), (COMBINE, 4, 0), (COMBINE, 2, 7), (COMBINE, 3, 8), (START, 2, 1), (LATE,),
    (COMBINE, 2, 6), (COMBINE, 2, 9), (COMBINE, 3, 6), (COMBINE, 3, 7), (START, 2, 2),
    (COMBINE, 2, 8), (COMBINE, 2, 3), (COMBINE, 2, 4), (START, 2, 3), (MIDDLE, 2, 0, -1),
    (MIDDLE, 2, 0, 1), (COMBINE, 0, 5), (COMBINE, 3, 4), (COMBINE, 1, 5), (COMBINE, 3, 3),
    (MIDDLE, 2, 1, -1), (MIDDLE, 2, 1, 1), (MIDDLE, 2, 2, -1), (MIDDLE, 2, 2, 1),
    (MIDDLE, 2, 3, -1), (MIDDLE, 2, 3, 1), (SUMMED, 2, 0), (SUMMED, 2, 1), (COMBINE, 3, 5),
    (COMBINE, 2, 5), (SUMMED, 2, 2), (SUMMED, 2, 3), (EARLY,), (COMBINE, 1, 1), (COMBINE, 0, 2),
    (COMBINE, 1, 2), (COMBINE, 0, 1), (COMBINE, 2, 2), (COMBINE, 3, 1), (COMBINE, 3, 2),
    (COMBINE, 2, 1), (COMBINE, 1, 0), (COMBINE, 0, 0), (COMBINE, 3, 0), (COMBINE, 2, 0),
]


def wrapped(n):
    n %= 4
    return n - 4 if n == 3 else n


def landing(hop):
    (da, db), ax, sg, _ = hop
    if ax == "a":
        da -= sg
    else:
        db -= sg
    return (wrapped(db), wrapped(da))


LANDS = [ORDER.index(landing(hop)) for hop in HOPS]
ARRIVALS = {o: [i for i, k in enumerate(LANDS) if ORDER[k] == o] for o in ORDER}
DUTIES = {o: [i for i, hop in enumerate(HOPS) if hop[0] == o] for o in ORDER}
PIECES = 2
DEEP = 128 // PIECES
HALF = DEEP // 2
SLOT, ARRIVED, GAINS, _at = {}, {}, {}, 0
for _k, _o in enumerate(ORDER):
    if DUTIES[_o]:
        GAINS[_k] = len(GAINS)
        _first = _at
        for _i in DUTIES[_o]:
            SLOT[_i] = _at
            _at += DEEP if HOPS[_i][3] is None else HALF
        ARRIVED[_k] = (_first, _at - _first)
ARRIVED_ROWS = _at
STRAIGHT_SUMS = ((0, 3),)
STRAIGHT_BLOCKS = (5,)


def scoped(f):
    return f


def turned(h, k):
    return ORDER.index(ORDER[k][::-1]) if h % 2 else k


def rows_of(h, k, part):
    start = turned(h, k) * 128 + h * DEEP
    return (start, DEEP) if part is None else (start + HALF * part, HALF)


def last_last(a, b):
    return lax.dot_general(a, b, (((1,), (1,)), ((), ())), preferred_element_type=F32)


def first_first(a, b):
    return lax.dot_general(a, b, (((0,), (0,)), ((), ())), preferred_element_type=F32)


def kernel(
    late_in, early_in, early_grad, pre_gain, post_gain, gate_w, up_w, down_w,
    gate_sum, up_sum, down_sum,
    late_out, early_out, gate_out, up_out, down_out,
    late_o, early_o, gate_o, up_o, down_o,
    late_v, early_v, grad_v, pre_v, post_v, gsum_v, usum_v, dsum_v,
    w_all, tok, tok_t, pre, dgate, dup, hid, part, pair, both, fwd, last, cot, hcot,
    gcot, ucot, grads, arrived, mixed, weighted,
    ag_s, ag_r, rs_s, rs_r, xa_s, xa_r, xr_s, xr_r, in_s,
):
    fs = lax.axis_index("fs")
    tp = lax.axis_index("tp")
    y, z = fs % 4, fs // 4
    par = (y + z) % 2
    core, x = tp % 2, tp // 2
    grad_scale = 1.0 / math.sqrt(8192.0)

    def fs_at(da, db):
        dy = (1 - par) * da + par * db
        dz = (1 - par) * db + par * da
        return ((z + dz + 4) % 4) * 4 + (y + dy + 4) % 4

    def torus(h, ax, sg):
        return (fs_at(sg, 0) if (ax == "a") == (h % 2 == 0) else fs_at(0, sg), tp)

    ring = {sg: (fs, ((x + sg + 4) % 4) * 2 + core) for sg in (1, -1, 2)}
    partner = (fs, x * 2 + 1 - core)
    columns = [pl.multiple_of(fs_at(*o) * 128, 128) for o in ORDER]

    fetched = []

    def fetch(src, dst):
        copy = pltpu.make_async_copy(src, dst, in_s.at[len(fetched)])
        copy.start()
        fetched.append(copy)
        return copy

    barrier = pltpu.get_barrier_semaphore()
    peers = [partner, ring[1], ring[-1], ring[2]] + [torus(0, ax, sg) for ax in "ab" for sg in (1, -1)]
    for peer in peers:
        pl.semaphore_signal(barrier, inc=1, device_id=peer, device_id_type=MESH)
    fetch_weights = [fetch(gate_w, w_all.at[0, pl.ds(0, 128)])]
    fetch_tokens = {1: fetch(early_in, early_v)}
    fetch_small = [fetch(pre_gain, pre_v)]
    fetch_weights.append(fetch(up_w, w_all.at[1, pl.ds(0, 128)]))
    fetch_tokens[0] = fetch(late_in, late_v)
    fetch_weights.append(fetch(down_w, w_all.at[2, pl.ds(0, 128)]))
    fetch_tokens[2] = fetch(early_grad, grad_v)
    fetch_small.append(fetch(post_gain, post_v))
    fetch_sums = [fetch(gate_sum, gsum_v), fetch(up_sum, usum_v), fetch(down_sum, dsum_v)]
    sums = ((gsum_v, gate_o, gate_out), (usum_v, up_o, up_out), (dsum_v, down_o, down_out))
    pl.semaphore_wait(barrier, len(peers))

    def send(src, dst, ss, rs, to):
        pltpu.make_async_remote_copy(
            src_ref=src, dst_ref=dst, send_sem=ss, recv_sem=rs,
            device_id=to, device_id_type=MESH,
        ).start()

    def arrive(dst, ss, rs):
        pltpu.make_async_remote_copy(
            src_ref=dst, dst_ref=dst, send_sem=ss, recv_sem=rs,
            device_id=partner, device_id_type=MESH,
        ).wait_recv()

    def pass_on(p, k):
        w, h = divmod(p, PIECES)
        for i in DUTIES[ORDER[k]]:
            _, ax, sg, q = HOPS[i]
            start, n = rows_of(h, k, q)
            there, _ = rows_of(h, LANDS[i], q)
            send(
                w_all.at[w, pl.ds(start, n)], w_all.at[w, pl.ds(there, n)],
                ag_s.at[p], ag_r.at[p, LANDS[i] - 1], torus(h, ax, sg),
            )

    @scoped
    def relay(p, k):
        w, h = divmod(p, PIECES)
        start, n = rows_of(h, k, None)
        arrive(w_all.at[w, pl.ds(start, n)], ag_s.at[p], ag_r.at[p, k - 1])
        pass_on(p, k)

    @scoped
    def own(p):
        if p % PIECES == 0:
            fetch_weights[p // PIECES].wait()
        pass_on(p, 0)

    def rows(j, row, n):
        if j < 2:
            return tok.at[j, pl.ds(row, n)]
        return cot.at[pl.ds(row, n), pl.ds(512 * (j - 2), 512)]

    def move(j, i, row, there, n, to):
        send(rows(j, row, n), rows(j, there, n), xa_s.at[j], xa_r.at[j, i], to)

    def come(j, i, row, n):
        arrive(rows(j, row, n), xa_s.at[j], xa_r.at[j, i])

    @scoped
    def spread(j):
        if j in STRAIGHT_BLOCKS:
            move(j, 2, 0, 128, 64, ring[2])
        move(j, 0, 0, 192, 64, ring[1])
        move(j, 1, 0, 64, 64, ring[-1])
        move(j, 3, 0, 256, 64, partner)

    @scoped
    def near(j, sg):
        at, there, part_at = (192, 128, 192) if sg == 1 else (64, 160, 96)
        come(j, (1 - sg) // 2, at, 64)
        if j not in STRAIGHT_BLOCKS:
            move(j, 2, part_at, there, 32, ring[sg])
        move(j, 3, at, 256 + at, 64, partner)

    @scoped
    def far(j):
        come(j, 2, 128, 64)
        move(j, 3, 128, 384, 64, partner)

    @scoped
    def full(j):
        come(j, 3, 256, 256)

    def pass_sum(v, g, i, row, n, ref, there, to):
        s = 4 * v + g
        send(
            both.at[v, g, pl.ds(row, n)], ref.at[v, g, pl.ds(there, n)],
            xr_s.at[s], xr_r.at[s, i], to,
        )

    def get_sum(v, g, i, ref, row, n):
        s = 4 * v + g
        arrive(ref.at[v, g, pl.ds(row, n)], xr_s.at[s], xr_r.at[s, i])

    def sum_pair(v, g):
        s = 4 * v + g
        send(part.at[v, g, pl.ds(256, 256)], pair.at[v, g], xr_s.at[s], xr_r.at[s, 0], partner)

    @scoped
    def start(v, g):
        get_sum(v, g, 0, pair, 0, 256)
        for r in (128, 64, 192, 0):
            both[v, g, r : r + 64] = (
                part[v, g, r : r + 64].astype(F32) + pair[v, g, r : r + 64].astype(F32)
            ).astype(BF)
            if r == 128 and (v, g) not in STRAIGHT_SUMS:
                pass_sum(v, g, 1, 128, 32, fwd, 0, ring[1])
                pass_sum(v, g, 2, 160, 32, fwd, 32, ring[-1])
            if (v, g) in STRAIGHT_SUMS and r:
                i, to = {128: (0, 2), 64: (1, 1), 192: (2, -1)}[r]
                pass_sum(v, g, 3, r, 64, last, 64 * i, ring[to])

    @scoped
    def middle(v, g, sg):
        i, r, t = (0, 64, 64) if sg == 1 else (1, 192, 224)
        get_sum(v, g, 1 + i, fwd, 32 * i, 32)
        both[v, g, t : t + 32] = (
            both[v, g, t : t + 32].astype(F32) + fwd[v, g, 32 * i : 32 * i + 32].astype(F32)
        ).astype(BF)
        pass_sum(v, g, 3, r, 64, last, 64 * i, ring[sg])

    @scoped
    def summed(v, g):
        n = 3 if (v, g) in STRAIGHT_SUMS else 2
        get_sum(v, g, 3, last, 0, 64 * n)
        total = both[v, g, :64].astype(F32)
        for i in range(n):
            total += last[v, g, 64 * i : 64 * i + 64].astype(F32)
        mixed[v, :, pl.ds(512 * g, 512)] = total.astype(BF)

    @scoped
    def combine(p, k):
        w, h = divmod(p, PIECES)
        if k in GAINS:
            first, n = ARRIVED[k]
            arrive(arrived.at[p, pl.ds(first, n)], rs_s.at[p], rs_r.at[p, GAINS[k]])
        for q in (0, 1):
            terms = []
            for i in DUTIES[ORDER[k]]:
                if HOPS[i][3] is None:
                    terms.append(SLOT[i] + HALF * q)
                elif HOPS[i][3] == q:
                    terms.append(SLOT[i])
            if terms:
                r, _ = rows_of(h, k, q)
                total = grads[w, r : r + HALF].astype(F32)
                for at in terms:
                    total += arrived[p, at : at + HALF].astype(F32)
                if k == 0:
                    olds, out, _ = sums[w]
                    out[r : r + HALF] = olds[r : r + HALF] + grad_scale * total
                else:
                    grads[w, r : r + HALF] = total.astype(BF)
        if k == 0:
            at = pl.ds(h * DEEP, DEEP)
            fetch(sums[w][1].at[at], sums[w][2].at[at])
        for i in ARRIVALS[ORDER[k]]:
            _, ax, sg, q = HOPS[i]
            r, n = rows_of(h, k, q)
            send(
                grads.at[w, pl.ds(r, n)], arrived.at[p, pl.ds(SLOT[i], n)],
                rs_s.at[p], rs_r.at[p, GAINS[ORDER.index(HOPS[i][0])]], torus(h, "b" if ax == "a" else "a", -sg),
            )

    def tiles(count, body):
        lax.fori_loop(0, count, lambda i, c: (body(i), c)[1], 0)

    @scoped
    def norm(m):
        if m == 1:
            fetch_small[0].wait()
        fetch_tokens[m].wait()
        source = (late_v, early_v)[m]
        values = source[...].astype(F32)
        inverse = lax.rsqrt(jnp.mean(values * values, axis=-1, keepdims=True) + NORM_EPS)
        for k, at in enumerate(columns):
            tok[m, 0:64, 128 * k : 128 * k + 128] = (
                source[:, pl.ds(at, 128)].astype(F32) * inverse * pre_v[:, pl.ds(at, 128)]
            ).astype(BF)

    @scoped
    def weigh():
        fetch_tokens[2].wait()
        fetch_small[1].wait()
        for copy in fetch_sums:
            copy.wait()
        for k, at in enumerate(columns):
            weighted[:, 128 * k : 128 * k + 128] = (
                0.5 * grad_v[:, pl.ds(at, 128)].astype(F32) * post_v[:, pl.ds(at, 128)]
            )

    @scoped
    def gate(m, t):
        r = 128 * t
        pre[m, r : r + 128] = jnp.dot(tok[m, r : r + 128], w_all[0], preferred_element_type=F32)

    @scoped
    def up(m, t):
        at = slice(128 * t, 128 * t + 128)
        ups = jnp.dot(tok[m, at], w_all[1], preferred_element_type=F32)
        gates = pre[m, at]
        s = jax.nn.sigmoid(gates)
        hid[m, at] = (gates * s * ups).astype(BF)
        if m == 1:
            dgate[at] = ups * s * (1.0 + gates * (1.0 - s))
            dup[at] = gates * s

    @scoped
    def down(v, g):
        def body(i):
            r = pl.multiple_of(256 - i * 256, 256)
            part[v, g, pl.ds(r, 256)] = last_last(
                hid[1 - v, pl.ds(r, 256)], w_all[2, pl.ds(512 * g, 512)]
            ).astype(BF)

        tiles(2, body)
        sum_pair(v, g)

    @scoped
    def back(g):
        def body(i):
            r = pl.multiple_of(i * 256, 256)
            part[2, g, pl.ds(r, 256)] = (
                last_last(gcot[pl.ds(r, 256)], w_all[0, pl.ds(512 * g, 512)])
                + last_last(ucot[pl.ds(r, 256)], w_all[1, pl.ds(512 * g, 512)])
            ).astype(BF)

        tiles(2, body)
        sum_pair(2, g)

    @scoped
    def cotangent():
        values = mixed[0].astype(F32)
        inverse = lax.rsqrt(jnp.mean(values * values, axis=-1, keepdims=True) + NORM_EPS)
        scaled = inverse**3 * jnp.mean(weighted[...] * values, axis=-1, keepdims=True)
        for g in (3, 2, 1, 0):
            at = slice(512 * g, 512 * g + 512)
            cot[0:64, at] = (
                inverse * weighted[:, at] - mixed[0, :, at].astype(F32) * scaled
            ).astype(BF)

    @scoped
    def hidden(g):
        def body(i):
            r = pl.multiple_of(i * 256, 256)
            term = jnp.dot(
                cot[pl.ds(r, 256), pl.ds(512 * g, 512)],
                w_all[2, pl.ds(512 * g, 512)],
                preferred_element_type=F32,
            )
            hcot[pl.ds(r, 256)] = hcot[pl.ds(r, 256)] + term if begun else term

        tiles(2, body)
        begun.append(g)

    @scoped
    def dgrad(g):
        grads[2, pl.ds(512 * g, 512)] = first_first(
            cot[:, pl.ds(512 * g, 512)], hid[1]
        ).astype(BF)

    @scoped
    def turn():
        for k in range(16):
            tok_t[128 * k : 128 * k + 128] = tok[1, :, 128 * k : 128 * k + 128].T

    @scoped
    def derive():
        gcot[...] = (hcot[...] * dgate[...]).astype(BF)
        ucot[...] = (hcot[...] * dup[...]).astype(BF)

    @scoped
    def wgrad(w, g):
        def body(i):
            r = pl.multiple_of(512 * g + i * 256, 256)
            grads[w, pl.ds(r, 256)] = jnp.dot(
                tok_t[pl.ds(r, 256)], (gcot, ucot)[w][...], preferred_element_type=F32
            ).astype(BF)

        tiles(2, body)

    @scoped
    def late_end():
        values = mixed[1].astype(F32)
        inverse = lax.rsqrt(jnp.mean(values * values, axis=-1, keepdims=True) + NORM_EPS)
        for k, at in enumerate(columns):
            late_o[:, pl.ds(at, 128)] = (
                late_v[:, pl.ds(at, 128)].astype(F32)
                + 0.5
                * mixed[1, :, 128 * k : 128 * k + 128].astype(F32)
                * inverse
                * post_v[:, pl.ds(at, 128)]
            ).astype(BF)
        fetch(late_o, late_out)

    @scoped
    def early_end():
        early = early_v[...].astype(F32)
        inverse = lax.rsqrt(jnp.mean(early * early, axis=-1, keepdims=True) + NORM_EPS)
        dots = jnp.zeros((64, 128), F32)
        for k, at in enumerate(columns):
            dots += (
                mixed[2, :, 128 * k : 128 * k + 128].astype(F32)
                * pre_v[:, pl.ds(at, 128)]
                * early_v[:, pl.ds(at, 128)].astype(F32)
            )
        slope = inverse**3 * (jnp.sum(dots, axis=-1, keepdims=True) * (1.0 / 2048.0))
        for k, at in enumerate(columns):
            early_o[:, pl.ds(at, 128)] = (
                grad_v[:, pl.ds(at, 128)].astype(F32)
                + inverse
                * (mixed[2, :, 128 * k : 128 * k + 128].astype(F32) * pre_v[:, pl.ds(at, 128)])
                - early_v[:, pl.ds(at, 128)].astype(F32) * slope
            ).astype(BF)
        fetch(early_o, early_out)

    begun = []
    steps = (
        own, relay, norm, spread, near, far, full, weigh, gate, up, down, back, start, middle,
        summed, turn, cotangent, hidden, dgrad, derive, wgrad, combine, late_end, early_end,
    )
    for name, *at in SCRIPT:
        steps[name](*at)

    def leave(ref, ss):
        pltpu.make_async_remote_copy(
            src_ref=ref, dst_ref=ref, send_sem=ss, recv_sem=ss,
            device_id=partner, device_id_type=MESH,
        ).wait_send()

    for p in range(3 * PIECES):
        leave(w_all.at[p // PIECES, pl.ds(0, 15 * DEEP)], ag_s.at[p])
        leave(grads.at[p // PIECES, pl.ds(0, 15 * DEEP)], rs_s.at[p])
    for j in range(6):
        leave(rows(j, 0, 448), xa_s.at[j])
    for s in range(12):
        leave(part.at[s // 4, s % 4, pl.ds(0, 448)], xr_s.at[s])
    for copy in fetched[11:]:
        copy.wait()


def hand_over(*refs):
    sources, targets, held, (in_s, out_s) = refs[:5], refs[5:10], refs[10:15], refs[15:]
    copies = [pltpu.make_async_copy(sources[i], held[i], in_s.at[i]) for i in range(5)]
    for copy in copies:
        copy.start()
    for i in range(5):
        copies[i].wait()
        copies[i] = pltpu.make_async_copy(held[i], targets[i], out_s.at[i])
        copies[i].start()
    for copy in copies:
        copy.wait()


def per_device(
    late_input,
    early_input,
    early_grad,
    pre_gain,
    post_gain,
    gate_weight,
    up_weight,
    down_weight,
    gate_sum,
    up_sum,
    down_gradient_sum,
):
    sem = pltpu.SemaphoreType.DMA
    vmem = pltpu.VMEM
    tokens = jax.ShapeDtypeStruct((64, 2048), BF)
    total = jax.ShapeDtypeStruct((128, 512), F32)
    results = pl.pallas_call(
        kernel,
        name="half_step",
        out_shape=(tokens, tokens, total, total, total),
        in_specs=[pl.BlockSpec(memory_space=pl.ANY)] * 11,
        out_specs=[pl.BlockSpec(memory_space=pl.ANY)] * 5,
        scratch_shapes=[
            vmem((64, 2048), BF),
            vmem((64, 2048), BF),
            vmem((128, 512), F32),
            vmem((128, 512), F32),
            vmem((128, 512), F32),
            vmem((64, 2048), BF),
            vmem((64, 2048), BF),
            vmem((64, 2048), BF),
            vmem((1, 2048), F32),
            vmem((1, 2048), F32),
            vmem((128, 512), F32),
            vmem((128, 512), F32),
            vmem((128, 512), F32),
            vmem((3, 2048, 512), BF),
            vmem((2, 512, 2048), BF),
            vmem((2048, 512), BF),
            vmem((2, 512, 512), F32),
            vmem((512, 512), F32),
            vmem((512, 512), F32),
            vmem((2, 512, 512), BF),
            vmem((3, 4, 512, 512), BF),
            vmem((3, 4, 256, 512), BF),
            vmem((3, 4, 256, 512), BF),
            vmem((3, 4, 64, 512), BF),
            vmem((3, 4, 192, 512), BF),
            vmem((512, 2048), BF),
            vmem((512, 512), F32),
            vmem((512, 512), BF),
            vmem((512, 512), BF),
            vmem((3, 2048, 512), BF),
            vmem((3 * PIECES, ARRIVED_ROWS, 512), BF),
            vmem((3, 64, 2048), BF),
            vmem((64, 2048), F32),
            sem((3 * PIECES,)),
            sem((3 * PIECES, 15)),
            sem((3 * PIECES,)),
            sem((3 * PIECES, len(GAINS))),
            sem((6,)),
            sem((6, 4)),
            sem((12,)),
            sem((12, 4)),
            sem((13 + 3 * PIECES,)),
        ],
        compiler_params=pltpu.CompilerParams(
            collective_id=0, has_side_effects=True, vmem_limit_bytes=67043328
        ),
    )(
        late_input, early_input, early_grad, pre_gain.reshape(1, -1), post_gain.reshape(1, -1),
        gate_weight, up_weight, down_weight, gate_sum, up_sum, down_gradient_sum,
    )
    return pl.pallas_call(
        hand_over,
        name="hand_over",
        out_shape=(tokens, tokens, total, total, total),
        in_specs=[pl.BlockSpec(memory_space=pl.ANY)] * 5,
        out_specs=[pl.BlockSpec(memory_space=pl.ANY)] * 5,
        scratch_shapes=[
            vmem((64, 2048), BF),
            vmem((64, 2048), BF),
            vmem((128, 512), F32),
            vmem((128, 512), F32),
            vmem((128, 512), F32),
            sem((5,)),
            sem((5,)),
        ],
        compiler_params=pltpu.CompilerParams(vmem_limit_bytes=67043328),
    )(*results)


def solution(mesh):
    rows, both = P(("fs", "tp"), None), P("fs", "tp")
    return jax.shard_map(
        per_device,
        mesh=mesh,
        in_specs=(rows,) * 3 + (P(), P()) + (both,) * 6,
        out_specs=(rows, rows, both, both, both),
        check_vma=False,
    )
```

```python
import math

import jax
import jax.numpy as jnp
from jax import lax
from jax.experimental import pallas as pl
from jax.experimental.pallas import tpu as pltpu
from jax.sharding import PartitionSpec as P

NORM_EPS = 1e-06
BF = jnp.bfloat16
F32 = jnp.float32
MESH = pl.DeviceIdType.MESH

ORDER = [
    (0, 0), (0, 1), (0, -1), (1, 0),
    (-1, 0), (2, 0), (1, 1), (1, -1),
    (-1, 1), (-1, -1), (0, 2), (1, 2),
    (-1, 2), (2, 1), (2, -1), (2, 2),
]
HOPS = (
    [((0, 0), ax, sg, None) for ax in "ab" for sg in (1, -1)]
    + [((2, 0), "b", sg, None) for sg in (1, -1)]
    + [((0, s), "a", sg, None) for s in (1, -1) for sg in (1, -1)]
    + [((0, s), "b", -s, (1 + s) // 2) for s in (1, -1)]
    + [((s, t), "b", -t, (1 + t) // 2) for s in (1, -1) for t in (1, -1)]
    + [((s, 0), "a", -s, (1 + s) // 2) for s in (1, -1)]
    + [((s, 2), "a", -s, (1 + s) // 2) for s in (1, -1)]
)


(
    OWN, RELAY, NORM, SPREAD, NEAR, FAR, FULL, WEIGH, GATE, UP, DOWN, BACK, START, MIDDLE,
    SUMMED, TURN, COT, HIDDEN, DGRAD, DERIVE, WGRAD, COMBINE, LATE, EARLY,
    PASS, GIVE,
) = range(26)
SCRIPT = [
    (NORM, 1), (SPREAD, 1), (OWN, 0), (PASS, 0, 0), (PASS, 0, 1), (PASS, 0, 2), (PASS, 0, 3),
    (OWN, 1), (NORM, 0), (PASS, 1, 0), (PASS, 1, 1), (PASS, 1, 2), (PASS, 1, 3), (OWN, 2),
    (SPREAD, 0), (WEIGH,), (PASS, 2, 0), (PASS, 2, 1), (PASS, 2, 2), (PASS, 2, 3), (PASS, 3, 2),
    (PASS, 3, 3), (PASS, 3, 0), (PASS, 3, 1), (RELAY, 0, 2), (RELAY, 0, 1), (RELAY, 0, 4),
    (RELAY, 0, 3), (PASS, 0, 6), (PASS, 0, 7), (PASS, 0, 11), (PASS, 0, 10), (PASS, 4, 2),
    (PASS, 4, 3), (RELAY, 1, 4), (RELAY, 1, 3), (RELAY, 1, 2), (RELAY, 1, 1), (PASS, 0, 8),
    (PASS, 0, 9), (PASS, 1, 6), (PASS, 1, 7), (RELAY, 2, 2), (RELAY, 2, 1), (RELAY, 2, 4),
    (RELAY, 2, 3), (PASS, 1, 11), (PASS, 1, 10), (PASS, 2, 6), (PASS, 2, 7), (PASS, 1, 8),
    (PASS, 1, 9), (NEAR, 1, -1), (NEAR, 1, 1), (RELAY, 3, 1), (RELAY, 3, 2), (RELAY, 3, 3),
    (RELAY, 3, 4), (RELAY, 0, 5), (PASS, 2, 8), (PASS, 2, 9), (PASS, 0, 4), (PASS, 0, 5),
    (RELAY, 0, 7), (RELAY, 0, 6), (PASS, 3, 11), (PASS, 3, 10), (PASS, 2, 11), (PASS, 2, 10),
    (RELAY, 0, 9), (RELAY, 0, 8), (PASS, 0, 17), (PASS, 0, 16), (PASS, 0, 13), (PASS, 0, 12),
    (RELAY, 1, 5), (RELAY, 1, 7), (RELAY, 1, 6), (PASS, 1, 4), (PASS, 1, 5), (PASS, 0, 15),
    (PASS, 0, 14), (PASS, 3, 6), (PASS, 3, 7), (RELAY, 2, 7), (RELAY, 2, 6), (RELAY, 1, 9),
    (RELAY, 1, 8), (PASS, 1, 13), (PASS, 1, 12), (NEAR, 0, -1), (NEAR, 0, 1), (PASS, 1, 15),
    (PASS, 1, 14), (PASS, 3, 8), (PASS, 3, 9), (RELAY, 2, 9), (RELAY, 2, 8), (RELAY, 0, 12),
    (RELAY, 0, 11), (PASS, 0, 19), (PASS, 0, 18), (RELAY, 3, 5), (RELAY, 2, 5), (PASS, 3, 4),
    (PASS, 3, 5), (PASS, 2, 4), (PASS, 2, 5), (RELAY, 0, 10), (RELAY, 0, 13), (FAR, 1),
    (RELAY, 0, 14), (PASS, 4, 0), (PASS, 4, 1), (PASS, 1, 17), (PASS, 1, 16), (RELAY, 4, 3),
    (RELAY, 4, 4), (RELAY, 1, 12), (RELAY, 1, 11), (PASS, 1, 19), (PASS, 1, 18), (RELAY, 1, 13),
    (RELAY, 3, 7), (RELAY, 3, 6), (FULL, 1), (TURN,), (PASS, 2, 12), (PASS, 2, 13), (PASS, 2, 16),
    (PASS, 2, 17), (RELAY, 1, 14), (PASS, 3, 13), (PASS, 3, 12), (PASS, 2, 15), (PASS, 2, 14),
    (FAR, 0), (RELAY, 0, 15), (RELAY, 3, 9), (RELAY, 3, 8), (PASS, 3, 15), (PASS, 3, 14),
    (PASS, 5, 0), (PASS, 5, 1), (PASS, 5, 2), (PASS, 5, 3), (RELAY, 3, 12), (RELAY, 3, 11),
    (RELAY, 2, 12), (RELAY, 2, 11), (FULL, 0), (PASS, 3, 19), (PASS, 3, 18), (RELAY, 1, 10),
    (PASS, 2, 19), (PASS, 2, 18), (PASS, 3, 17), (PASS, 3, 16), (RELAY, 4, 2), (RELAY, 4, 1),
    (RELAY, 1, 15), (GATE, 1, 0), (GATE, 1, 1), (PASS, 4, 10), (PASS, 4, 11), (PASS, 4, 6),
    (PASS, 4, 7), (RELAY, 2, 10), (RELAY, 2, 13), (GATE, 1, 2), (GATE, 1, 3), (RELAY, 2, 14),
    (RELAY, 3, 13), (GATE, 0, 0), (PASS, 4, 8), (PASS, 4, 9), (RELAY, 3, 14), (GATE, 0, 1),
    (GATE, 0, 2), (RELAY, 5, 1), (PASS, 5, 6), (PASS, 5, 7), (RELAY, 5, 2), (GATE, 0, 3),
    (PASS, 5, 10), (PASS, 5, 11), (PASS, 5, 8), (PASS, 5, 9), (RELAY, 3, 15), (RELAY, 5, 3),
    (RELAY, 5, 4), (PASS, 4, 17), (PASS, 4, 16), (RELAY, 2, 15), (RELAY, 3, 10), (UP, 1, 0),
    (UP, 1, 1), (PASS, 5, 16), (PASS, 5, 17), (RELAY, 4, 5), (UP, 1, 2), (PASS, 4, 4),
    (PASS, 4, 5), (RELAY, 4, 6), (RELAY, 4, 7), (UP, 1, 3), (DOWN, 0, 0), (PASS, 4, 12),
    (PASS, 4, 13), (UP, 0, 0), (RELAY, 4, 8), (RELAY, 4, 9), (RELAY, 5, 6), (PASS, 5, 12),
    (RELAY, 5, 7), (PASS, 5, 13), (UP, 0, 1), (PASS, 4, 14), (PASS, 4, 15), (RELAY, 5, 5),
    (PASS, 5, 4), (PASS, 5, 5), (UP, 0, 2), (RELAY, 4, 10), (UP, 0, 3), (RELAY, 5, 8),
    (PASS, 5, 14), (RELAY, 5, 9), (PASS, 5, 15), (START, 0, 0), (DOWN, 1, 0), (RELAY, 5, 10),
    (DOWN, 0, 1), (DOWN, 1, 1), (RELAY, 4, 11), (PASS, 4, 18), (RELAY, 4, 12), (PASS, 4, 19),
    (RELAY, 5, 13), (DOWN, 1, 2), (RELAY, 4, 13), (RELAY, 4, 14), (RELAY, 5, 11), (PASS, 5, 18),
    (RELAY, 5, 12), (PASS, 5, 19), (DOWN, 0, 3), (MIDDLE, 0, 0, -1), (MIDDLE, 0, 0, 1),
    (START, 0, 1), (RELAY, 5, 14), (DOWN, 0, 2), (START, 0, 3), (RELAY, 4, 15), (START, 0, 2),
    (RELAY, 5, 15), (DOWN, 0, 4), (DOWN, 1, 3), (SUMMED, 0, 0), (START, 0, 4), (MIDDLE, 0, 1, -1),
    (MIDDLE, 0, 1, 1), (MIDDLE, 0, 2, 1), (MIDDLE, 0, 2, -1), (SUMMED, 0, 3), (SUMMED, 0, 4),
    (SUMMED, 0, 1), (SUMMED, 0, 2), (COT,), (SPREAD, 2), (SPREAD, 3), (NEAR, 2, -1), (NEAR, 2, 1),
    (SPREAD, 4), (NEAR, 3, 1), (NEAR, 3, -1), (SPREAD, 5), (FAR, 2), (FULL, 2), (DGRAD, 0),
    (GIVE, 4, 18), (GIVE, 4, 19), (GIVE, 5, 18), (GIVE, 5, 19), (FAR, 3), (NEAR, 4, 1),
    (NEAR, 4, -1), (SPREAD, 6), (FULL, 3), (DGRAD, 1), (GIVE, 4, 12), (GIVE, 4, 13),
    (GIVE, 4, 14), (GIVE, 4, 15), (NEAR, 5, 1), (NEAR, 5, -1), (START, 1, 0), (START, 1, 1),
    (START, 1, 2), (START, 1, 3), (COMBINE, 5, 11), (GIVE, 5, 5), (COMBINE, 5, 12), (GIVE, 5, 4),
    (FAR, 4), (FULL, 4), (DGRAD, 2), (GIVE, 5, 12), (GIVE, 5, 13), (GIVE, 5, 14), (GIVE, 5, 15),
    (NEAR, 6, -1), (NEAR, 6, 1), (COMBINE, 4, 11), (GIVE, 4, 5), (COMBINE, 4, 12), (GIVE, 4, 4),
    (COMBINE, 4, 9), (HIDDEN, 3), (GIVE, 4, 16), (GIVE, 4, 17), (FAR, 5), (COMBINE, 5, 5),
    (GIVE, 5, 10), (GIVE, 5, 11), (MIDDLE, 1, 0, 1), (MIDDLE, 1, 0, -1), (GIVE, 4, 8),
    (MIDDLE, 1, 1, 1), (MIDDLE, 1, 1, -1), (FULL, 5), (DGRAD, 3), (GIVE, 5, 16), (GIVE, 5, 17),
    (COMBINE, 4, 6), (GIVE, 4, 7), (COMBINE, 4, 7), (COMBINE, 4, 8), (MIDDLE, 1, 2, -1),
    (MIDDLE, 1, 2, 1), (HIDDEN, 2), (GIVE, 4, 6), (GIVE, 4, 9), (COMBINE, 5, 6), (GIVE, 5, 7),
    (COMBINE, 5, 7), (GIVE, 5, 6), (MIDDLE, 1, 3, -1), (MIDDLE, 1, 3, 1), (COMBINE, 5, 8),
    (GIVE, 5, 9), (COMBINE, 5, 9), (GIVE, 5, 8), (COMBINE, 4, 5), (FAR, 6), (GIVE, 4, 10),
    (GIVE, 4, 11), (FULL, 6), (DGRAD, 4), (COMBINE, 4, 3), (GIVE, 4, 3), (COMBINE, 4, 4),
    (GIVE, 4, 2), (COMBINE, 5, 3), (GIVE, 5, 3), (COMBINE, 5, 4), (GIVE, 5, 2), (HIDDEN, 0),
    (HIDDEN, 1), (COMBINE, 5, 1), (GIVE, 5, 1), (DERIVE,), (WGRAD, 0, 3), (GIVE, 0, 18),
    (GIVE, 0, 19), (GIVE, 1, 19), (GIVE, 0, 13), (GIVE, 1, 14), (GIVE, 1, 15), (WGRAD, 0, 2),
    (GIVE, 1, 18), (GIVE, 0, 15), (GIVE, 1, 12), (GIVE, 1, 13), (COMBINE, 5, 2), (WGRAD, 0, 1),
    (GIVE, 0, 12), (GIVE, 0, 16), (GIVE, 0, 17), (GIVE, 1, 17), (COMBINE, 4, 1), (COMBINE, 4, 2),
    (WGRAD, 0, 0), (GIVE, 0, 14), (GIVE, 4, 0), (GIVE, 4, 1), (GIVE, 5, 0), (WGRAD, 1, 3),
    (GIVE, 3, 18), (WGRAD, 1, 2), (GIVE, 2, 18), (GIVE, 2, 19), (GIVE, 3, 19), (GIVE, 2, 12),
    (COMBINE, 0, 11), (COMBINE, 0, 12), (COMBINE, 1, 12), (WGRAD, 1, 1), (GIVE, 0, 4),
    (GIVE, 0, 5), (GIVE, 1, 4), (GIVE, 3, 12), (COMBINE, 0, 7), (COMBINE, 1, 8), (COMBINE, 1, 9),
    (WGRAD, 1, 0), (GIVE, 3, 14), (COMBINE, 0, 9), (COMBINE, 1, 11), (COMBINE, 1, 6),
    (COMBINE, 1, 7), (SUMMED, 1, 0), (SUMMED, 1, 1), (SUMMED, 1, 2), (SUMMED, 1, 3), (BACK, 0),
    (GIVE, 1, 5), (GIVE, 2, 13), (GIVE, 2, 14), (GIVE, 3, 13), (GIVE, 1, 16), (COMBINE, 0, 3),
    (COMBINE, 0, 4), (COMBINE, 0, 6), (COMBINE, 0, 8), (GIVE, 2, 15), (GIVE, 3, 15),
    (COMBINE, 1, 4), (BACK, 1), (GIVE, 2, 16), (GIVE, 2, 17), (GIVE, 3, 16), (GIVE, 3, 17),
    (COMBINE, 3, 11), (BACK, 2), (GIVE, 3, 5), (GIVE, 0, 6), (GIVE, 1, 6), (GIVE, 1, 7),
    (COMBINE, 2, 11), (COMBINE, 2, 12), (COMBINE, 2, 6), (COMBINE, 3, 12), (START, 2, 0),
    (BACK, 3), (GIVE, 2, 4), (GIVE, 2, 5), (GIVE, 3, 4), (GIVE, 0, 7), (COMBINE, 0, 5),
    (COMBINE, 3, 6), (COMBINE, 3, 8), (START, 2, 1), (COMBINE, 4, 0), (COMBINE, 5, 0), (LATE,),
    (COMBINE, 2, 7), (COMBINE, 2, 8), (COMBINE, 3, 7), (START, 2, 2), (GIVE, 0, 10),
    (COMBINE, 1, 3), (GIVE, 0, 9), (GIVE, 0, 8), (GIVE, 0, 11), (COMBINE, 1, 5), (COMBINE, 2, 9),
    (COMBINE, 3, 9), (GIVE, 1, 9), (START, 2, 3), (COMBINE, 3, 3), (GIVE, 1, 8), (COMBINE, 2, 3),
    (COMBINE, 2, 4), (COMBINE, 3, 4), (MIDDLE, 2, 0, -1), (MIDDLE, 2, 0, 1), (GIVE, 1, 10),
    (GIVE, 1, 11), (GIVE, 3, 7), (GIVE, 2, 7), (GIVE, 2, 6), (GIVE, 3, 6), (MIDDLE, 2, 1, -1),
    (MIDDLE, 2, 1, 1), (MIDDLE, 2, 2, -1), (MIDDLE, 2, 2, 1), (GIVE, 3, 9), (GIVE, 2, 9),
    (GIVE, 2, 8), (GIVE, 3, 8), (COMBINE, 3, 5), (COMBINE, 2, 5), (MIDDLE, 2, 3, -1),
    (MIDDLE, 2, 3, 1), (COMBINE, 0, 1), (GIVE, 2, 10), (GIVE, 3, 10), (GIVE, 3, 11),
    (GIVE, 2, 11), (COMBINE, 0, 2), (SUMMED, 2, 0), (GIVE, 0, 3), (GIVE, 0, 1), (GIVE, 0, 0),
    (GIVE, 0, 2), (COMBINE, 1, 1), (COMBINE, 1, 2), (SUMMED, 2, 1), (GIVE, 1, 1), (GIVE, 1, 3),
    (GIVE, 1, 2), (GIVE, 1, 0), (SUMMED, 2, 2), (GIVE, 2, 3), (GIVE, 3, 3), (GIVE, 3, 2),
    (GIVE, 2, 2), (COMBINE, 2, 1), (COMBINE, 3, 1), (COMBINE, 2, 2), (COMBINE, 3, 2),
    (SUMMED, 2, 3), (EARLY,), (GIVE, 2, 0), (GIVE, 2, 1), (GIVE, 3, 0), (GIVE, 3, 1),
    (COMBINE, 0, 0), (COMBINE, 1, 0), (COMBINE, 2, 0), (COMBINE, 3, 0),
]


def wrapped(n):
    n %= 4
    return n - 4 if n == 3 else n


def landing(hop):
    (da, db), ax, sg, _ = hop
    if ax == "a":
        da -= sg
    else:
        db -= sg
    return (wrapped(db), wrapped(da))


LANDS = [ORDER.index(landing(hop)) for hop in HOPS]
ARRIVALS = {o: [i for i, k in enumerate(LANDS) if ORDER[k] == o] for o in ORDER}
DUTIES = {o: [i for i, hop in enumerate(HOPS) if hop[0] == o] for o in ORDER}
PIECES = 2
DEEP = 128 // PIECES
HALF = DEEP // 2
SLOT, ARRIVED, GAINS, _at = {}, {}, {}, 0
for _k, _o in enumerate(ORDER):
    if DUTIES[_o]:
        GAINS[_k] = len(GAINS)
        _first = _at
        for _i in DUTIES[_o]:
            SLOT[_i] = _at
            _at += DEEP if HOPS[_i][3] is None else HALF
        ARRIVED[_k] = (_first, _at - _first)
ARRIVED_ROWS = _at
STRAIGHT_SUMS = ((0, 3), (0, 4))
STRAIGHT_BLOCKS = (2, 3)
SUMS = (
    ((0, 5), (5, 4), (9, 4), (13, 2), (15, 1)),
    ((0, 4), (4, 4), (8, 4), (12, 4)),
    ((0, 4), (4, 4), (8, 4), (12, 4)),
)
BLOCKS = ((15, 1), (13, 2), (9, 4), (5, 4), (0, 5))
SUM_AT = (0, len(SUMS[0]), len(SUMS[0]) + len(SUMS[1]))


def lanes(group):
    return pl.ds(128 * group[0], 128 * group[1])


def scoped(f):
    return f


def turned(h, k):
    return ORDER.index(ORDER[k][::-1]) if h % 2 else k


def rows_of(h, k, part):
    start = turned(h, k) * 128 + h * DEEP
    return (start, DEEP) if part is None else (start + HALF * part, HALF)


def last_last(a, b):
    return lax.dot_general(a, b, (((1,), (1,)), ((), ())), preferred_element_type=F32)


def first_first(a, b):
    return lax.dot_general(a, b, (((0,), (0,)), ((), ())), preferred_element_type=F32)


def kernel(
    late_in, early_in, early_grad, pre_gain, post_gain, gate_w, up_w, down_w,
    gate_sum, up_sum, down_sum,
    late_out, early_out, gate_out, up_out, down_out,
    late_v, early_v, grad_v, pre_v, post_v, gsum_v, usum_v, dsum_v,
    w_all, tok, tok_t, pre, dgate, dup, hid, part, pair, both, fwd, last, cot, hcot,
    gcot, ucot, grads, arrived, mixed, weighted,
    ag_s, ag_r, rs_s, rs_r, xa_s, xa_r, xr_s, xr_r, in_s,
):
    fs = lax.axis_index("fs")
    tp = lax.axis_index("tp")
    y, z = fs % 4, fs // 4
    par = (y + z) % 2
    core, x = tp % 2, tp // 2
    grad_scale = 1.0 / math.sqrt(8192.0)

    def fs_at(da, db):
        dy = (1 - par) * da + par * db
        dz = (1 - par) * db + par * da
        return ((z + dz + 4) % 4) * 4 + (y + dy + 4) % 4

    def torus(h, ax, sg):
        return (fs_at(sg, 0) if (ax == "a") == (h % 2 == 0) else fs_at(0, sg), tp)

    ring = {sg: (fs, ((x + sg + 4) % 4) * 2 + core) for sg in (1, -1, 2)}
    partner = (fs, x * 2 + 1 - core)
    columns = [pl.multiple_of(fs_at(*o) * 128, 128) for o in ORDER]

    fetched = []

    def fetch(src, dst):
        copy = pltpu.make_async_copy(src, dst, in_s.at[len(fetched)])
        copy.start()
        fetched.append(copy)
        return copy

    barrier = pltpu.get_barrier_semaphore()
    peers = [partner, ring[1], ring[-1], ring[2]] + [torus(0, ax, sg) for ax in "ab" for sg in (1, -1)]
    for peer in peers:
        pl.semaphore_signal(barrier, inc=1, device_id=peer, device_id_type=MESH)
    fetch_weights = [fetch(gate_w, w_all.at[0, pl.ds(0, 128)])]
    fetch_tokens = {1: fetch(early_in, early_v)}
    fetch_small = [fetch(pre_gain, pre_v)]
    fetch_weights.append(fetch(up_w, w_all.at[1, pl.ds(0, 128)]))
    fetch_tokens[0] = fetch(late_in, late_v)
    fetch_weights.append(fetch(down_w, w_all.at[2, pl.ds(0, 128)]))
    fetch_tokens[2] = fetch(early_grad, grad_v)
    fetch_small.append(fetch(post_gain, post_v))
    fetch_sums = [fetch(gate_sum, gsum_v), fetch(up_sum, usum_v), fetch(down_sum, dsum_v)]
    sums = ((gsum_v, gate_out), (usum_v, up_out), (dsum_v, down_out))
    pl.semaphore_wait(barrier, len(peers))

    def send(src, dst, ss, rs, to):
        pltpu.make_async_remote_copy(
            src_ref=src, dst_ref=dst, send_sem=ss, recv_sem=rs,
            device_id=to, device_id_type=MESH,
        ).start()

    def arrive(dst, ss, rs):
        pltpu.make_async_remote_copy(
            src_ref=dst, dst_ref=dst, send_sem=ss, recv_sem=rs,
            device_id=partner, device_id_type=MESH,
        ).wait_recv()

    @scoped
    def pass_on(p, i):
        w, h = divmod(p, PIECES)
        offset, ax, sg, q = HOPS[i]
        start, n = rows_of(h, ORDER.index(offset), q)
        there, _ = rows_of(h, LANDS[i], q)
        send(
            w_all.at[w, pl.ds(start, n)], w_all.at[w, pl.ds(there, n)],
            ag_s, ag_r.at[p, LANDS[i] - 1], torus(h, ax, sg),
        )

    @scoped
    def relay(p, k):
        w, h = divmod(p, PIECES)
        start, n = rows_of(h, k, None)
        arrive(w_all.at[w, pl.ds(start, n)], ag_s, ag_r.at[p, k - 1])

    @scoped
    def own(w):
        fetch_weights[w].wait()

    def rows(j, row, n):
        if j < 2:
            return tok.at[j, pl.ds(row, n)]
        return cot.at[pl.ds(row, n), lanes(BLOCKS[j - 2])]

    def move(j, i, row, there, n, to):
        send(rows(j, row, n), rows(j, there, n), xa_s.at[min(j // 2, 1)], xa_r.at[j, i], to)

    def come(j, i, row, n):
        arrive(rows(j, row, n), xa_s.at[min(j // 2, 1)], xa_r.at[j, i])

    @scoped
    def spread(j):
        move(j, 0, 0, 192, 64, ring[1])
        move(j, 1, 0, 64, 64, ring[-1])
        if j in STRAIGHT_BLOCKS:
            move(j, 2, 0, 128, 64, ring[2])
        move(j, 3, 0, 256, 64, partner)

    @scoped
    def near(j, sg):
        at, there, part_at = (192, 128, 192) if sg == 1 else (64, 160, 96)
        come(j, (1 - sg) // 2, at, 64)
        if j not in STRAIGHT_BLOCKS:
            move(j, 2, part_at, there, 32, ring[sg])
        move(j, 3, at, 256 + at, 64, partner)

    @scoped
    def far(j):
        come(j, 2, 128, 64)
        move(j, 3, 128, 384, 64, partner)

    @scoped
    def full(j):
        come(j, 3, 256, 256)

    def pass_sum(v, g, i, source, row, n, ref, there, to):
        at = lanes(SUMS[v][g])
        send(
            source.at[v, pl.ds(row, n), at], ref.at[v, pl.ds(there, n), at],
            xr_s, xr_r.at[SUM_AT[v] + g, i], to,
        )

    def get_sum(v, g, i, ref, row, n):
        arrive(ref.at[v, pl.ds(row, n), lanes(SUMS[v][g])], xr_s, xr_r.at[SUM_AT[v] + g, i])

    @scoped
    def start(v, g):
        at = lanes(SUMS[v][g])
        get_sum(v, g, 0, pair, 0, 256)
        for r in (64, 192, 128, 0):
            if r == 64 and (v, g) not in STRAIGHT_SUMS:
                r = 128
            elif r == 128 and (v, g) not in STRAIGHT_SUMS:
                r = 64
            both[v, r : r + 64, at] = (
                part[v, r : r + 64, at].astype(F32) + pair[v, r : r + 64, at].astype(F32)
            ).astype(BF)
            if (v, g) in STRAIGHT_SUMS and r:
                i, to = {128: (0, 2), 64: (1, 1), 192: (2, -1)}[r]
                pass_sum(v, g, 3, both, r, 64, last, 64 * i, ring[to])
            elif r == 128:
                pass_sum(v, g, 1, both, 128, 32, fwd, 0, ring[1])
                pass_sum(v, g, 2, both, 160, 32, fwd, 32, ring[-1])

    @scoped
    def middle(v, g, sg):
        at = lanes(SUMS[v][g])
        i, r, t = (0, 64, 64) if sg == 1 else (1, 192, 224)
        get_sum(v, g, 1 + i, fwd, 32 * i, 32)
        both[v, t : t + 32, at] = (
            both[v, t : t + 32, at].astype(F32) + fwd[v, 32 * i : 32 * i + 32, at].astype(F32)
        ).astype(BF)
        pass_sum(v, g, 3, both, r, 64, last, 64 * i, ring[sg])

    @scoped
    def summed(v, g):
        at = lanes(SUMS[v][g])
        n = 3 if (v, g) in STRAIGHT_SUMS else 2
        get_sum(v, g, 3, last, 0, 64 * n)
        total = both[v, :64, at].astype(F32)
        for i in range(n):
            total += last[v, 64 * i : 64 * i + 64, at].astype(F32)
        mixed[v, :, at] = total.astype(BF)

    @scoped
    def combine(p, k):
        w, h = divmod(p, PIECES)
        if k in GAINS:
            first, n = ARRIVED[k]
            arrive(arrived.at[p, pl.ds(first, n)], rs_s, rs_r.at[p, GAINS[k]])
        for q in (0, 1):
            terms = []
            for i in DUTIES[ORDER[k]]:
                if HOPS[i][3] is None:
                    terms.append(SLOT[i] + HALF * q)
                elif HOPS[i][3] == q:
                    terms.append(SLOT[i])
            if terms:
                r, _ = rows_of(h, k, q)
                total = grads[w, r : r + HALF].astype(F32)
                for at in terms:
                    total += arrived[p, at : at + HALF].astype(F32)
                if k == 0:
                    olds, out = sums[w]
                    out[r : r + HALF] = olds[r : r + HALF] + grad_scale * total
                else:
                    grads[w, r : r + HALF] = total.astype(BF)

    @scoped
    def give(p, i):
        w, h = divmod(p, PIECES)
        offset, ax, sg, q = HOPS[i]
        r, n = rows_of(h, LANDS[i], q)
        send(
            grads.at[w, pl.ds(r, n)], arrived.at[p, pl.ds(SLOT[i], n)],
            rs_s, rs_r.at[p, GAINS[ORDER.index(offset)]],
            torus(h, "b" if ax == "a" else "a", -sg),
        )

    def tiles(count, body):
        lax.fori_loop(0, count, lambda i, c: (body(i), c)[1], 0)

    @scoped
    def norm(m):
        if m == 1:
            fetch_small[0].wait()
        fetch_tokens[m].wait()
        source = (late_v, early_v)[m]
        values = source[...].astype(F32)
        inverse = lax.rsqrt(jnp.mean(values * values, axis=-1, keepdims=True) + NORM_EPS)
        for k, at in enumerate(columns):
            tok[m, 0:64, 128 * k : 128 * k + 128] = (
                source[:, pl.ds(at, 128)].astype(F32) * inverse * pre_v[:, pl.ds(at, 128)]
            ).astype(BF)

    @scoped
    def weigh():
        fetch_tokens[2].wait()
        fetch_small[1].wait()
        for copy in fetch_sums:
            copy.wait()
        for k, at in enumerate(columns):
            weighted[:, 128 * k : 128 * k + 128] = (
                0.5 * grad_v[:, pl.ds(at, 128)].astype(F32) * post_v[:, pl.ds(at, 128)]
            )

    @scoped
    def gate(m, t):
        r = 128 * t
        pre[m, r : r + 128] = jnp.dot(tok[m, r : r + 128], w_all[0], preferred_element_type=F32)

    @scoped
    def up(m, t):
        at = slice(128 * t, 128 * t + 128)
        ups = jnp.dot(tok[m, at], w_all[1], preferred_element_type=F32)
        gates = pre[m, at]
        s = jax.nn.sigmoid(gates)
        hid[m, at] = (gates * s * ups).astype(BF)
        if m == 1:
            dgate[at] = ups * s * (1.0 + gates * (1.0 - s))
            dup[at] = gates * s

    @scoped
    def down(v, g):
        first, n = SUMS[v][g]

        def body(i):
            r = pl.multiple_of(256 - i * 256, 256)
            part[v, pl.ds(r, 256), lanes(SUMS[v][g])] = last_last(
                hid[1 - v, pl.ds(r, 256)], w_all[2, pl.ds(128 * first, 128 * n)]
            ).astype(BF)

        tiles(2, body)
        pass_sum(v, g, 0, part, 256, 256, pair, 0, partner)

    @scoped
    def back(g):
        first, n = SUMS[2][g]

        def body(i):
            r = pl.multiple_of(i * 256, 256)
            part[2, pl.ds(r, 256), lanes(SUMS[2][g])] = (
                last_last(gcot[pl.ds(r, 256)], w_all[0, pl.ds(128 * first, 128 * n)])
                + last_last(ucot[pl.ds(r, 256)], w_all[1, pl.ds(128 * first, 128 * n)])
            ).astype(BF)

        tiles(2, body)
        pass_sum(2, g, 0, part, 256, 256, pair, 0, partner)

    @scoped
    def cotangent():
        values = mixed[0].astype(F32)
        inverse = lax.rsqrt(jnp.mean(values * values, axis=-1, keepdims=True) + NORM_EPS)
        scaled = inverse**3 * jnp.mean(weighted[...] * values, axis=-1, keepdims=True)
        for g in (3, 2, 1, 0):
            at = slice(512 * g, 512 * g + 512)
            cot[0:64, at] = (
                inverse * weighted[:, at] - mixed[0, :, at].astype(F32) * scaled
            ).astype(BF)

    @scoped
    def hidden(g):
        def body(i):
            r = pl.multiple_of(i * 256, 256)
            term = jnp.dot(
                cot[pl.ds(r, 256), pl.ds(512 * g, 512)],
                w_all[2, pl.ds(512 * g, 512)],
                preferred_element_type=F32,
            )
            hcot[pl.ds(r, 256)] = hcot[pl.ds(r, 256)] + term if begun else term

        tiles(2, body)
        begun.append(g)

    @scoped
    def dgrad(g):
        first, n = BLOCKS[g]
        grads[2, pl.ds(128 * first, 128 * n)] = first_first(
            cot[:, lanes(BLOCKS[g])], hid[1]
        ).astype(BF)

    @scoped
    def turn():
        for k in range(16):
            tok_t[128 * k : 128 * k + 128] = tok[1, :, 128 * k : 128 * k + 128].T

    @scoped
    def derive():
        gcot[...] = (hcot[...] * dgate[...]).astype(BF)
        ucot[...] = (hcot[...] * dup[...]).astype(BF)

    @scoped
    def wgrad(w, g):
        def body(i):
            r = pl.multiple_of(512 * g + i * 256, 256)
            grads[w, pl.ds(r, 256)] = jnp.dot(
                tok_t[pl.ds(r, 256)], (gcot, ucot)[w][...], preferred_element_type=F32
            ).astype(BF)

        tiles(2, body)

    @scoped
    def late_end():
        values = mixed[1].astype(F32)
        inverse = lax.rsqrt(jnp.mean(values * values, axis=-1, keepdims=True) + NORM_EPS)
        for k, at in enumerate(columns):
            late_out[:, pl.ds(at, 128)] = (
                late_v[:, pl.ds(at, 128)].astype(F32)
                + 0.5
                * mixed[1, :, 128 * k : 128 * k + 128].astype(F32)
                * inverse
                * post_v[:, pl.ds(at, 128)]
            ).astype(BF)

    @scoped
    def early_end():
        early = early_v[...].astype(F32)
        inverse = lax.rsqrt(jnp.mean(early * early, axis=-1, keepdims=True) + NORM_EPS)
        dots = jnp.zeros((64, 128), F32)
        for k, at in enumerate(columns):
            dots += (
                mixed[2, :, 128 * k : 128 * k + 128].astype(F32)
                * pre_v[:, pl.ds(at, 128)]
                * early_v[:, pl.ds(at, 128)].astype(F32)
            )
        slope = inverse**3 * (jnp.sum(dots, axis=-1, keepdims=True) * (1.0 / 2048.0))
        for k, at in enumerate(columns):
            early_out[:, pl.ds(at, 128)] = (
                grad_v[:, pl.ds(at, 128)].astype(F32)
                + inverse
                * (mixed[2, :, 128 * k : 128 * k + 128].astype(F32) * pre_v[:, pl.ds(at, 128)])
                - early_v[:, pl.ds(at, 128)].astype(F32) * slope
            ).astype(BF)

    begun = []
    steps = (
        own, relay, norm, spread, near, far, full, weigh, gate, up, down, back, start, middle,
        summed, turn, cotangent, hidden, dgrad, derive, wgrad, combine, late_end, early_end,
        pass_on, give,
    )
    for name, *at in SCRIPT:
        steps[name](*at)

    def leave(ref, ss):
        pltpu.make_async_remote_copy(
            src_ref=ref, dst_ref=ref, send_sem=ss, recv_sem=ss,
            device_id=partner, device_id_type=MESH,
        ).wait_send()

    leave(w_all.reshape(3 * 2048, 512).at[pl.ds(0, 3 * 15 * 128)], ag_s)
    leave(grads.reshape(3 * 2048, 512).at[pl.ds(0, 3 * 15 * 128)], rs_s)
    leave(tok.reshape(1024, 2048).at[pl.ds(0, 2 * 448)], xa_s.at[0])
    leave(cot.at[pl.ds(0, 448)], xa_s.at[1])
    leave(part.reshape(3 * 512, 2048).at[pl.ds(0, 3 * 448)], xr_s)


def hand_over(*refs):
    copies = [pltpu.make_async_copy(refs[i], refs[5 + i], refs[10].at[i]) for i in range(5)]
    for copy in copies:
        copy.start()
    for copy in copies:
        copy.wait()


def per_device(
    late_input,
    early_input,
    early_grad,
    pre_gain,
    post_gain,
    gate_weight,
    up_weight,
    down_weight,
    gate_sum,
    up_sum,
    down_gradient_sum,
):
    sem = pltpu.SemaphoreType.DMA
    vmem = pltpu.VMEM
    tokens = jax.ShapeDtypeStruct((64, 2048), BF)
    total = jax.ShapeDtypeStruct((128, 512), F32)
    results = pl.pallas_call(
        kernel,
        name="half_step",
        out_shape=(vmem((64, 2048), BF),) * 2 + (vmem((128, 512), F32),) * 3,
        in_specs=[pl.BlockSpec(memory_space=pl.ANY)] * 11,
        out_specs=[pl.BlockSpec(memory_space=vmem)] * 5,
        scratch_shapes=[
            vmem((64, 2048), BF),
            vmem((64, 2048), BF),
            vmem((64, 2048), BF),
            vmem((1, 2048), F32),
            vmem((1, 2048), F32),
            vmem((128, 512), F32),
            vmem((128, 512), F32),
            vmem((128, 512), F32),
            vmem((3, 2048, 512), BF),
            vmem((2, 512, 2048), BF),
            vmem((2048, 512), BF),
            vmem((2, 512, 512), F32),
            vmem((512, 512), F32),
            vmem((512, 512), F32),
            vmem((2, 512, 512), BF),
            vmem((3, 512, 2048), BF),
            vmem((3, 256, 2048), BF),
            vmem((3, 256, 2048), BF),
            vmem((3, 64, 2048), BF),
            vmem((3, 192, 2048), BF),
            vmem((512, 2048), BF),
            vmem((512, 512), F32),
            vmem((512, 512), BF),
            vmem((512, 512), BF),
            vmem((3, 2048, 512), BF),
            vmem((3 * PIECES, ARRIVED_ROWS, 512), BF),
            vmem((3, 64, 2048), BF),
            vmem((64, 2048), F32),
            sem,
            sem((3 * PIECES, 15)),
            sem,
            sem((3 * PIECES, len(GAINS))),
            sem((2,)),
            sem((2 + len(BLOCKS), 4)),
            sem,
            sem((SUM_AT[2] + len(SUMS[2]), 4)),
            sem((11,)),
        ],
        compiler_params=pltpu.CompilerParams(
            collective_id=0, has_side_effects=True, vmem_limit_bytes=60 * 2**20
        ),
    )(
        late_input, early_input, early_grad, pre_gain.reshape(1, -1), post_gain.reshape(1, -1),
        gate_weight, up_weight, down_weight, gate_sum, up_sum, down_gradient_sum,
    )
    return pl.pallas_call(
        hand_over,
        name="hand_over",
        out_shape=(tokens, tokens, total, total, total),
        in_specs=[pl.BlockSpec(memory_space=vmem)] * 5,
        out_specs=[pl.BlockSpec(memory_space=pl.ANY)] * 5,
        scratch_shapes=[sem((5,))],
        compiler_params=pltpu.CompilerParams(vmem_limit_bytes=4 * 2**20),
    )(*results)


def solution(mesh):
    rows, both = P(("fs", "tp"), None), P("fs", "tp")
    return jax.shard_map(
        per_device,
        mesh=mesh,
        in_specs=(rows,) * 3 + (P(), P()) + (both,) * 6,
        out_specs=(rows, rows, both, both, both),
        check_vma=False,
    )
```

```python
import math

import jax
import jax.numpy as jnp
from jax import lax
from jax.experimental import pallas as pl
from jax.experimental.pallas import tpu as pltpu
from jax.sharding import PartitionSpec as P

NORM_EPS = 1e-06
BF = jnp.bfloat16
F32 = jnp.float32
MESH = pl.DeviceIdType.MESH

ORDER = [
    (0, 0), (0, 1), (0, -1), (1, 0),
    (-1, 0), (2, 0), (1, 1), (1, -1),
    (-1, 1), (-1, -1), (0, 2), (1, 2),
    (-1, 2), (2, 1), (2, -1), (2, 2),
]
HOPS = (
    [((0, 0), ax, sg, None) for ax in "ab" for sg in (1, -1)]
    + [((2, 0), "b", sg, None) for sg in (1, -1)]
    + [((0, s), "a", sg, None) for s in (1, -1) for sg in (1, -1)]
    + [((0, s), "b", -s, (1 + s) // 2) for s in (1, -1)]
    + [((s, t), "b", -t, (1 + t) // 2) for s in (1, -1) for t in (1, -1)]
    + [((s, 0), "a", -s, (1 + s) // 2) for s in (1, -1)]
    + [((s, 2), "a", -s, (1 + s) // 2) for s in (1, -1)]
)


(
    OWN, RELAY, NORM, SPREAD, NEAR, FAR, FULL, WEIGH, GATE, UP, DOWN, BACK, START, MIDDLE,
    SUMMED, TURN, COT, HIDDEN, DGRAD, DERIVE, WGRAD, COMBINE, LATE, EARLY,
    PASS, GIVE,
) = range(26)
SCRIPT = [
    (NORM, 1), (SPREAD, 1), (OWN, 0), (PASS, 0, 0), (PASS, 0, 1), (PASS, 0, 2), (PASS, 0, 3),
    (NORM, 0), (PASS, 1, 0), (PASS, 1, 1), (PASS, 1, 2), (PASS, 1, 3), (OWN, 1), (OWN, 2),
    (SPREAD, 0), (WEIGH,), (PASS, 2, 0), (PASS, 2, 1), (PASS, 2, 2), (PASS, 2, 3), (PASS, 3, 2),
    (PASS, 3, 3), (PASS, 3, 0), (PASS, 3, 1), (RELAY, 0, 2), (RELAY, 0, 1), (RELAY, 0, 4),
    (RELAY, 0, 3), (PASS, 0, 6), (PASS, 0, 7), (PASS, 0, 11), (PASS, 0, 10), (PASS, 4, 2),
    (PASS, 4, 3), (RELAY, 1, 4), (RELAY, 1, 3), (RELAY, 1, 2), (RELAY, 1, 1), (PASS, 1, 11),
    (PASS, 1, 10), (PASS, 0, 8), (PASS, 0, 9), (PASS, 1, 6), (PASS, 1, 7), (RELAY, 2, 2),
    (RELAY, 2, 1), (RELAY, 2, 4), (RELAY, 2, 3), (PASS, 2, 6), (PASS, 2, 7), (PASS, 2, 11),
    (PASS, 2, 10), (NEAR, 1, 1), (NEAR, 1, -1), (RELAY, 3, 1), (RELAY, 3, 2), (RELAY, 3, 3),
    (RELAY, 3, 4), (PASS, 1, 8), (PASS, 1, 9), (RELAY, 0, 5), (PASS, 3, 11), (PASS, 3, 10),
    (RELAY, 0, 7), (RELAY, 0, 6), (PASS, 2, 8), (PASS, 2, 9), (PASS, 0, 4), (PASS, 0, 5),
    (RELAY, 1, 5), (PASS, 1, 4), (PASS, 1, 5), (PASS, 0, 13), (PASS, 0, 12), (RELAY, 0, 9),
    (RELAY, 0, 8), (RELAY, 1, 7), (RELAY, 1, 6), (PASS, 0, 15), (PASS, 0, 14), (RELAY, 2, 5),
    (PASS, 0, 17), (PASS, 0, 16), (PASS, 2, 4), (PASS, 2, 5), (RELAY, 2, 7), (RELAY, 2, 6),
    (PASS, 1, 13), (PASS, 1, 12), (NEAR, 0, 1), (NEAR, 0, -1), (RELAY, 1, 8), (RELAY, 1, 9),
    (RELAY, 3, 5), (PASS, 1, 15), (PASS, 1, 14), (PASS, 3, 6), (PASS, 3, 7), (PASS, 3, 4),
    (PASS, 3, 5), (RELAY, 2, 9), (RELAY, 2, 8), (RELAY, 0, 12), (RELAY, 0, 11), (PASS, 3, 8),
    (PASS, 3, 9), (RELAY, 0, 13), (PASS, 0, 19), (PASS, 0, 18), (FAR, 1), (RELAY, 1, 12),
    (RELAY, 1, 11), (RELAY, 0, 14), (PASS, 4, 0), (PASS, 4, 1), (PASS, 1, 19), (PASS, 1, 18),
    (RELAY, 4, 3), (RELAY, 4, 4), (RELAY, 0, 10), (PASS, 1, 17), (PASS, 1, 16), (RELAY, 1, 13),
    (RELAY, 2, 12), (RELAY, 2, 11), (FULL, 1), (TURN,), (PASS, 2, 18), (PASS, 2, 19),
    (PASS, 2, 12), (PASS, 2, 13), (RELAY, 1, 14), (PASS, 2, 17), (PASS, 2, 16), (PASS, 2, 15),
    (PASS, 2, 14), (FAR, 0), (RELAY, 3, 7), (RELAY, 3, 6), (PASS, 5, 2), (PASS, 5, 3),
    (PASS, 5, 0), (PASS, 5, 1), (RELAY, 3, 12), (RELAY, 3, 11), (RELAY, 0, 15), (RELAY, 3, 9),
    (RELAY, 3, 8), (FULL, 0), (PASS, 3, 13), (PASS, 3, 12), (PASS, 3, 19), (PASS, 3, 18),
    (RELAY, 1, 15), (PASS, 3, 15), (PASS, 3, 14), (PASS, 3, 17), (PASS, 3, 16), (RELAY, 4, 2),
    (RELAY, 4, 1), (RELAY, 1, 10), (GATE, 1, 0), (GATE, 1, 1), (PASS, 4, 10), (PASS, 4, 11),
    (PASS, 4, 6), (PASS, 4, 7), (RELAY, 2, 13), (RELAY, 2, 15), (GATE, 1, 2), (GATE, 1, 3),
    (RELAY, 2, 10), (RELAY, 2, 14), (GATE, 0, 0), (PASS, 4, 8), (PASS, 4, 9), (GATE, 0, 1),
    (GATE, 0, 2), (RELAY, 5, 1), (PASS, 5, 6), (PASS, 5, 7), (RELAY, 5, 2), (RELAY, 5, 3),
    (RELAY, 5, 4), (GATE, 0, 3), (PASS, 5, 10), (PASS, 5, 11), (PASS, 5, 8), (PASS, 5, 9),
    (RELAY, 3, 13), (RELAY, 3, 15), (PASS, 4, 17), (PASS, 4, 16), (RELAY, 3, 14), (RELAY, 3, 10),
    (UP, 1, 0), (UP, 1, 1), (PASS, 5, 16), (PASS, 5, 17), (RELAY, 4, 5), (UP, 1, 2), (PASS, 4, 4),
    (PASS, 4, 5), (RELAY, 4, 6), (RELAY, 4, 7), (UP, 1, 3), (DOWN, 0, 0), (PASS, 4, 12),
    (PASS, 4, 13), (UP, 0, 0), (RELAY, 4, 8), (RELAY, 4, 9), (RELAY, 5, 6), (PASS, 5, 12),
    (RELAY, 5, 7), (PASS, 5, 13), (UP, 0, 1), (PASS, 4, 14), (PASS, 4, 15), (RELAY, 5, 5),
    (PASS, 5, 4), (PASS, 5, 5), (UP, 0, 2), (RELAY, 4, 10), (UP, 0, 3), (RELAY, 5, 8),
    (PASS, 5, 14), (RELAY, 5, 9), (PASS, 5, 15), (START, 0, 0), (DOWN, 1, 0), (RELAY, 5, 10),
    (DOWN, 0, 1), (DOWN, 1, 1), (RELAY, 4, 11), (PASS, 4, 18), (RELAY, 4, 12), (PASS, 4, 19),
    (RELAY, 5, 13), (DOWN, 1, 2), (RELAY, 4, 13), (RELAY, 4, 14), (RELAY, 5, 11), (PASS, 5, 18),
    (RELAY, 5, 12), (PASS, 5, 19), (DOWN, 0, 3), (MIDDLE, 0, 0, 1), (MIDDLE, 0, 0, -1),
    (START, 0, 1), (RELAY, 5, 14), (DOWN, 0, 2), (START, 0, 3), (RELAY, 4, 15), (START, 0, 2),
    (RELAY, 5, 15), (DOWN, 0, 4), (DOWN, 1, 3), (SUMMED, 0, 0), (START, 0, 4), (MIDDLE, 0, 1, 1),
    (MIDDLE, 0, 1, -1), (MIDDLE, 0, 2, 1), (MIDDLE, 0, 2, -1), (SUMMED, 0, 3), (SUMMED, 0, 4),
    (SUMMED, 0, 1), (SUMMED, 0, 2), (COT,), (SPREAD, 2), (SPREAD, 3), (NEAR, 2, 1), (NEAR, 2, -1),
    (SPREAD, 4), (NEAR, 3, 1), (NEAR, 3, -1), (SPREAD, 5), (FAR, 2), (FULL, 2), (DGRAD, 0),
    (GIVE, 4, 18), (GIVE, 4, 19), (GIVE, 5, 18), (GIVE, 5, 19), (FAR, 3), (NEAR, 4, 1),
    (NEAR, 4, -1), (SPREAD, 6), (FULL, 3), (DGRAD, 1), (GIVE, 4, 12), (GIVE, 4, 13),
    (GIVE, 4, 14), (GIVE, 4, 15), (NEAR, 5, 1), (NEAR, 5, -1), (COMBINE, 5, 11), (GIVE, 5, 5),
    (COMBINE, 5, 12), (GIVE, 5, 4), (FAR, 4), (FULL, 4), (DGRAD, 2), (GIVE, 5, 12), (GIVE, 5, 13),
    (GIVE, 5, 14), (GIVE, 5, 15), (NEAR, 6, 1), (NEAR, 6, -1), (COMBINE, 4, 9), (COMBINE, 4, 11),
    (GIVE, 4, 5), (COMBINE, 4, 12), (GIVE, 4, 4), (HIDDEN, 3), (GIVE, 4, 16), (GIVE, 4, 17),
    (FAR, 5), (START, 1, 0), (COMBINE, 5, 5), (START, 1, 1), (GIVE, 5, 10), (GIVE, 5, 11),
    (START, 1, 2), (START, 1, 3), (GIVE, 4, 8), (FULL, 5), (DGRAD, 3), (GIVE, 5, 16),
    (GIVE, 5, 17), (COMBINE, 4, 6), (GIVE, 4, 7), (COMBINE, 4, 7), (COMBINE, 4, 8), (HIDDEN, 2),
    (GIVE, 4, 6), (GIVE, 4, 9), (COMBINE, 5, 6), (GIVE, 5, 7), (FAR, 6), (COMBINE, 5, 7),
    (GIVE, 5, 6), (COMBINE, 5, 8), (GIVE, 5, 9), (COMBINE, 5, 9), (GIVE, 5, 8), (COMBINE, 4, 5),
    (MIDDLE, 1, 0, 1), (MIDDLE, 1, 0, -1), (MIDDLE, 1, 1, 1), (FULL, 6), (DGRAD, 4),
    (GIVE, 4, 10), (GIVE, 4, 11), (COMBINE, 4, 3), (COMBINE, 4, 4), (HIDDEN, 0), (GIVE, 4, 3),
    (GIVE, 4, 2), (COMBINE, 5, 3), (GIVE, 5, 3), (COMBINE, 5, 4), (GIVE, 5, 2), (HIDDEN, 1),
    (DERIVE,), (WGRAD, 0, 3), (GIVE, 0, 12), (GIVE, 0, 13), (GIVE, 0, 18), (GIVE, 0, 19),
    (GIVE, 1, 14), (GIVE, 1, 15), (COMBINE, 5, 1), (WGRAD, 0, 2), (GIVE, 0, 14), (GIVE, 0, 15),
    (GIVE, 1, 12), (GIVE, 1, 13), (WGRAD, 0, 1), (GIVE, 1, 18), (GIVE, 1, 19), (GIVE, 0, 16),
    (GIVE, 0, 17), (COMBINE, 5, 2), (WGRAD, 0, 0), (GIVE, 1, 16), (GIVE, 1, 17), (COMBINE, 4, 1),
    (GIVE, 4, 1), (COMBINE, 4, 2), (GIVE, 4, 0), (WGRAD, 1, 3), (GIVE, 2, 12), (GIVE, 2, 13),
    (WGRAD, 1, 2), (GIVE, 2, 14), (GIVE, 2, 15), (GIVE, 2, 18), (GIVE, 2, 19), (COMBINE, 0, 11),
    (COMBINE, 0, 12), (WGRAD, 1, 1), (GIVE, 3, 12), (GIVE, 3, 13), (GIVE, 3, 18), (GIVE, 3, 19),
    (COMBINE, 0, 6), (COMBINE, 0, 7), (COMBINE, 1, 8), (COMBINE, 1, 9), (BACK, 0), (GIVE, 3, 14),
    (GIVE, 3, 15), (GIVE, 0, 5), (GIVE, 0, 4), (COMBINE, 0, 8), (COMBINE, 0, 9), (COMBINE, 1, 6),
    (COMBINE, 1, 7), (BACK, 1), (GIVE, 2, 16), (GIVE, 2, 17), (GIVE, 3, 16), (GIVE, 3, 17),
    (GIVE, 0, 7), (GIVE, 0, 6), (COMBINE, 0, 3), (COMBINE, 0, 4), (COMBINE, 1, 3),
    (COMBINE, 1, 4), (COMBINE, 1, 11), (COMBINE, 1, 12), (BACK, 2), (GIVE, 1, 7), (GIVE, 1, 6),
    (COMBINE, 2, 6), (COMBINE, 2, 7), (START, 2, 0), (BACK, 3), (GIVE, 1, 5), (GIVE, 1, 4),
    (GIVE, 1, 9), (GIVE, 1, 8), (COMBINE, 2, 8), (COMBINE, 2, 9), (COMBINE, 2, 11),
    (COMBINE, 2, 12), (COMBINE, 3, 6), (COMBINE, 3, 7), (COMBINE, 3, 11), (COMBINE, 3, 12),
    (START, 2, 1), (WGRAD, 1, 0), (GIVE, 3, 5), (GIVE, 3, 4), (COMBINE, 3, 8), (COMBINE, 3, 9),
    (START, 2, 2), (MIDDLE, 1, 1, -1), (MIDDLE, 1, 2, 1), (MIDDLE, 1, 2, -1), (MIDDLE, 1, 3, 1),
    (MIDDLE, 1, 3, -1), (SUMMED, 1, 0), (COMBINE, 4, 0), (GIVE, 2, 5), (COMBINE, 2, 3),
    (GIVE, 2, 4), (COMBINE, 2, 4), (COMBINE, 0, 5), (START, 2, 3), (GIVE, 0, 9), (GIVE, 0, 8),
    (COMBINE, 3, 3), (COMBINE, 3, 4), (MIDDLE, 2, 0, 1), (MIDDLE, 2, 0, -1), (GIVE, 0, 10),
    (GIVE, 0, 11), (GIVE, 2, 7), (GIVE, 2, 6), (GIVE, 3, 7), (MIDDLE, 2, 1, 1), (GIVE, 3, 6),
    (MIDDLE, 2, 1, -1), (COMBINE, 1, 5), (MIDDLE, 2, 2, 1), (MIDDLE, 2, 2, -1), (GIVE, 1, 10),
    (GIVE, 1, 11), (GIVE, 3, 9), (GIVE, 3, 8), (GIVE, 2, 9), (GIVE, 2, 8), (COMBINE, 3, 5),
    (SUMMED, 1, 1), (GIVE, 0, 3), (GIVE, 0, 2), (COMBINE, 2, 5), (GIVE, 3, 10), (GIVE, 3, 11),
    (SUMMED, 1, 2), (COMBINE, 0, 1), (COMBINE, 0, 2), (GIVE, 0, 1), (GIVE, 0, 0), (GIVE, 2, 10),
    (GIVE, 2, 11), (MIDDLE, 2, 3, 1), (GIVE, 2, 3), (GIVE, 2, 2), (SUMMED, 1, 3), (LATE,),
    (GIVE, 1, 3), (GIVE, 1, 2), (COMBINE, 1, 1), (COMBINE, 1, 2), (MIDDLE, 2, 3, -1),
    (GIVE, 1, 1), (GIVE, 1, 0), (GIVE, 3, 3), (GIVE, 3, 2), (SUMMED, 2, 0), (GIVE, 5, 1),
    (COMBINE, 3, 1), (GIVE, 5, 0), (COMBINE, 3, 2), (SUMMED, 2, 1), (COMBINE, 2, 1), (GIVE, 2, 1),
    (COMBINE, 2, 2), (GIVE, 2, 0), (GIVE, 3, 1), (COMBINE, 0, 0), (GIVE, 3, 0), (SUMMED, 2, 2),
    (SUMMED, 2, 3), (EARLY,), (COMBINE, 1, 0), (COMBINE, 5, 0), (COMBINE, 2, 0), (COMBINE, 3, 0),
]


def wrapped(n):
    n %= 4
    return n - 4 if n == 3 else n


def landing(hop):
    (da, db), ax, sg, _ = hop
    if ax == "a":
        da -= sg
    else:
        db -= sg
    return (wrapped(db), wrapped(da))


LANDS = [ORDER.index(landing(hop)) for hop in HOPS]
ARRIVALS = {o: [i for i, k in enumerate(LANDS) if ORDER[k] == o] for o in ORDER}
DUTIES = {o: [i for i, hop in enumerate(HOPS) if hop[0] == o] for o in ORDER}
PIECES = 2
DEEP = 128 // PIECES
HALF = DEEP // 2
SLOT, ARRIVED, GAINS, _at = {}, {}, {}, 0
for _k, _o in enumerate(ORDER):
    if DUTIES[_o]:
        GAINS[_k] = len(GAINS)
        _first = _at
        for _i in DUTIES[_o]:
            SLOT[_i] = _at
            _at += DEEP if HOPS[_i][3] is None else HALF
        ARRIVED[_k] = (_first, _at - _first)
ARRIVED_ROWS = _at
STRAIGHT_SUMS = ((0, 3), (0, 4))
STRAIGHT_BLOCKS = (2, 3)
SUMS = (
    ((0, 5), (5, 4), (9, 4), (13, 2), (15, 1)),
    ((0, 4), (4, 4), (8, 4), (12, 4)),
    ((0, 4), (4, 4), (8, 4), (12, 4)),
)
BLOCKS = ((15, 1), (13, 2), (9, 4), (5, 4), (0, 5))
SUM_AT = (0, len(SUMS[0]), len(SUMS[0]) + len(SUMS[1]))


def lanes(group):
    return pl.ds(128 * group[0], 128 * group[1])


def scoped(f):
    return f


def turned(h, k):
    return ORDER.index(ORDER[k][::-1]) if h % 2 else k


def rows_of(h, k, part):
    start = turned(h, k) * 128 + h * DEEP
    return (start, DEEP) if part is None else (start + HALF * part, HALF)


def last_last(a, b):
    return lax.dot_general(a, b, (((1,), (1,)), ((), ())), preferred_element_type=F32)


def first_first(a, b):
    return lax.dot_general(a, b, (((0,), (0,)), ((), ())), preferred_element_type=F32)


def kernel(
    late_in, early_in, early_grad, pre_gain, post_gain, gate_w, up_w, down_w,
    gate_sum, up_sum, down_sum,
    late_out, early_out, gate_out, up_out, down_out,
    late_v, early_v, grad_v, pre_v, post_v, gsum_v, usum_v, dsum_v,
    w_all, tok, tok_t, pre, dgate, dup, hid, part, pair, both, fwd, last, cot, hcot,
    gcot, ucot, grads, arrived, mixed, weighted,
    ag_s, ag_r, rs_s, rs_r, xa_s, xa_r, xr_s, xr_r, in_s,
):
    fs = lax.axis_index("fs")
    tp = lax.axis_index("tp")
    y, z = fs % 4, fs // 4
    par = (y + z) % 2
    core, x = tp % 2, tp // 2
    grad_scale = 1.0 / math.sqrt(8192.0)

    def fs_at(da, db):
        dy = (1 - par) * da + par * db
        dz = (1 - par) * db + par * da
        return ((z + dz + 4) % 4) * 4 + (y + dy + 4) % 4

    def torus(h, ax, sg):
        return (fs_at(sg, 0) if (ax == "a") == (h % 2 == 0) else fs_at(0, sg), tp)

    ring = {sg: (fs, ((x + sg + 4) % 4) * 2 + core) for sg in (1, -1, 2)}
    partner = (fs, x * 2 + 1 - core)
    columns = [pl.multiple_of(fs_at(*o) * 128, 128) for o in ORDER]

    fetched = []

    def fetch(src, dst):
        copy = pltpu.make_async_copy(src, dst, in_s.at[len(fetched)])
        copy.start()
        fetched.append(copy)
        return copy

    barrier = pltpu.get_barrier_semaphore()
    peers = [partner, ring[1], ring[-1], ring[2]] + [torus(0, ax, sg) for ax in "ab" for sg in (1, -1)]
    for peer in peers:
        pl.semaphore_signal(barrier, inc=1, device_id=peer, device_id_type=MESH)
    fetch_weights = [fetch(gate_w, w_all.at[0, pl.ds(0, 128)])]
    fetch_tokens = {1: fetch(early_in, early_v)}
    fetch_small = [fetch(pre_gain, pre_v)]
    fetch_weights.append(fetch(up_w, w_all.at[1, pl.ds(0, 128)]))
    fetch_tokens[0] = fetch(late_in, late_v)
    fetch_weights.append(fetch(down_w, w_all.at[2, pl.ds(0, 128)]))
    fetch_tokens[2] = fetch(early_grad, grad_v)
    fetch_small.append(fetch(post_gain, post_v))
    fetch_sums = [fetch(gate_sum, gsum_v), fetch(up_sum, usum_v), fetch(down_sum, dsum_v)]
    sums = ((gsum_v, gate_out), (usum_v, up_out), (dsum_v, down_out))
    pl.semaphore_wait(barrier, len(peers))

    def send(src, dst, ss, rs, to):
        pltpu.make_async_remote_copy(
            src_ref=src, dst_ref=dst, send_sem=ss, recv_sem=rs,
            device_id=to, device_id_type=MESH,
        ).start()

    def arrive(dst, ss, rs):
        pltpu.make_async_remote_copy(
            src_ref=dst, dst_ref=dst, send_sem=ss, recv_sem=rs,
            device_id=partner, device_id_type=MESH,
        ).wait_recv()

    @scoped
    def pass_on(p, i):
        w, h = divmod(p, PIECES)
        offset, ax, sg, q = HOPS[i]
        start, n = rows_of(h, ORDER.index(offset), q)
        there, _ = rows_of(h, LANDS[i], q)
        send(
            w_all.at[w, pl.ds(start, n)], w_all.at[w, pl.ds(there, n)],
            ag_s, ag_r.at[p, LANDS[i] - 1], torus(h, ax, sg),
        )

    @scoped
    def relay(p, k):
        w, h = divmod(p, PIECES)
        start, n = rows_of(h, k, None)
        arrive(w_all.at[w, pl.ds(start, n)], ag_s, ag_r.at[p, k - 1])

    @scoped
    def own(w):
        fetch_weights[w].wait()

    def rows(j, row, n):
        if j < 2:
            return tok.at[j, pl.ds(row, n)]
        return cot.at[pl.ds(row, n), lanes(BLOCKS[j - 2])]

    def move(j, i, row, there, n, to):
        send(rows(j, row, n), rows(j, there, n), xa_s.at[min(j // 2, 1)], xa_r.at[j, i], to)

    def come(j, i, row, n):
        arrive(rows(j, row, n), xa_s.at[min(j // 2, 1)], xa_r.at[j, i])

    @scoped
    def spread(j):
        move(j, 0, 0, 192, 64, ring[1])
        move(j, 1, 0, 64, 64, ring[-1])
        if j in STRAIGHT_BLOCKS:
            move(j, 2, 0, 128, 64, ring[2])
        move(j, 3, 0, 256, 64, partner)

    @scoped
    def near(j, sg):
        at, there, part_at = (192, 128, 192) if sg == 1 else (64, 160, 96)
        come(j, (1 - sg) // 2, at, 64)
        if j not in STRAIGHT_BLOCKS:
            move(j, 2, part_at, there, 32, ring[sg])
        move(j, 3, at, 256 + at, 64, partner)

    @scoped
    def far(j):
        come(j, 2, 128, 64)
        move(j, 3, 128, 384, 64, partner)

    @scoped
    def full(j):
        come(j, 3, 256, 256)

    def pass_sum(v, g, i, source, row, n, ref, there, to):
        at = lanes(SUMS[v][g])
        send(
            source.at[v, pl.ds(row, n), at], ref.at[v, pl.ds(there, n), at],
            xr_s, xr_r.at[SUM_AT[v] + g, i], to,
        )

    def get_sum(v, g, i, ref, row, n):
        arrive(ref.at[v, pl.ds(row, n), lanes(SUMS[v][g])], xr_s, xr_r.at[SUM_AT[v] + g, i])

    @scoped
    def start(v, g):
        at = lanes(SUMS[v][g])
        get_sum(v, g, 0, pair, 0, 256)
        for r in (64, 192, 128, 0):
            if r == 64 and (v, g) not in STRAIGHT_SUMS:
                r = 128
            elif r == 128 and (v, g) not in STRAIGHT_SUMS:
                r = 64
            both[v, r : r + 64, at] = (
                part[v, r : r + 64, at].astype(F32) + pair[v, r : r + 64, at].astype(F32)
            ).astype(BF)
            if (v, g) in STRAIGHT_SUMS and r:
                i, to = {128: (0, 2), 64: (1, 1), 192: (2, -1)}[r]
                pass_sum(v, g, 3, both, r, 64, last, 64 * i, ring[to])
            elif r == 128:
                pass_sum(v, g, 1, both, 128, 32, fwd, 0, ring[1])
                pass_sum(v, g, 2, both, 160, 32, fwd, 32, ring[-1])

    @scoped
    def middle(v, g, sg):
        at = lanes(SUMS[v][g])
        i, r, t = (0, 64, 64) if sg == 1 else (1, 192, 224)
        get_sum(v, g, 1 + i, fwd, 32 * i, 32)
        both[v, t : t + 32, at] = (
            both[v, t : t + 32, at].astype(F32) + fwd[v, 32 * i : 32 * i + 32, at].astype(F32)
        ).astype(BF)
        pass_sum(v, g, 3, both, r, 64, last, 64 * i, ring[sg])

    @scoped
    def summed(v, g):
        at = lanes(SUMS[v][g])
        n = 3 if (v, g) in STRAIGHT_SUMS else 2
        get_sum(v, g, 3, last, 0, 64 * n)
        total = both[v, :64, at].astype(F32)
        for i in range(n):
            total += last[v, 64 * i : 64 * i + 64, at].astype(F32)
        mixed[v, :, at] = total.astype(BF)

    @scoped
    def combine(p, k):
        w, h = divmod(p, PIECES)
        if k in GAINS:
            first, n = ARRIVED[k]
            arrive(arrived.at[p, pl.ds(first, n)], rs_s, rs_r.at[p, GAINS[k]])
        for q in (0, 1):
            terms = []
            for i in DUTIES[ORDER[k]]:
                if HOPS[i][3] is None:
                    terms.append(SLOT[i] + HALF * q)
                elif HOPS[i][3] == q:
                    terms.append(SLOT[i])
            if terms:
                r, _ = rows_of(h, k, q)
                total = grads[w, r : r + HALF].astype(F32)
                for at in terms:
                    total += arrived[p, at : at + HALF].astype(F32)
                if k == 0:
                    olds, out = sums[w]
                    out[r : r + HALF] = olds[r : r + HALF] + grad_scale * total
                else:
                    grads[w, r : r + HALF] = total.astype(BF)

    @scoped
    def give(p, i):
        w, h = divmod(p, PIECES)
        offset, ax, sg, q = HOPS[i]
        r, n = rows_of(h, LANDS[i], q)
        send(
            grads.at[w, pl.ds(r, n)], arrived.at[p, pl.ds(SLOT[i], n)],
            rs_s, rs_r.at[p, GAINS[ORDER.index(offset)]],
            torus(h, "b" if ax == "a" else "a", -sg),
        )

    def tiles(count, body):
        lax.fori_loop(0, count, lambda i, c: (body(i), c)[1], 0)

    @scoped
    def norm(m):
        if m == 1:
            fetch_small[0].wait()
        fetch_tokens[m].wait()
        source = (late_v, early_v)[m]
        values = source[...].astype(F32)
        inverse = lax.rsqrt(jnp.mean(values * values, axis=-1, keepdims=True) + NORM_EPS)
        for k, at in enumerate(columns):
            tok[m, 0:64, 128 * k : 128 * k + 128] = (
                source[:, pl.ds(at, 128)].astype(F32) * inverse * pre_v[:, pl.ds(at, 128)]
            ).astype(BF)

    @scoped
    def weigh():
        fetch_tokens[2].wait()
        fetch_small[1].wait()
        for copy in fetch_sums:
            copy.wait()
        for k, at in enumerate(columns):
            weighted[:, 128 * k : 128 * k + 128] = (
                0.5 * grad_v[:, pl.ds(at, 128)].astype(F32) * post_v[:, pl.ds(at, 128)]
            )

    @scoped
    def gate(m, t):
        r = 128 * t
        pre[m, r : r + 128] = jnp.dot(tok[m, r : r + 128], w_all[0], preferred_element_type=F32)

    @scoped
    def up(m, t):
        at = slice(128 * t, 128 * t + 128)
        ups = jnp.dot(tok[m, at], w_all[1], preferred_element_type=F32)
        gates = pre[m, at]
        s = jax.nn.sigmoid(gates)
        hid[m, at] = (gates * s * ups).astype(BF)
        if m == 1:
            dgate[at] = ups * s * (1.0 + gates * (1.0 - s))
            dup[at] = gates * s

    @scoped
    def down(v, g):
        first, n = SUMS[v][g]

        def body(i):
            r = pl.multiple_of(256 - i * 256, 256)
            part[v, pl.ds(r, 256), lanes(SUMS[v][g])] = last_last(
                hid[1 - v, pl.ds(r, 256)], w_all[2, pl.ds(128 * first, 128 * n)]
            ).astype(BF)

        tiles(2, body)
        pass_sum(v, g, 0, part, 256, 256, pair, 0, partner)

    @scoped
    def back(g):
        first, n = SUMS[2][g]

        def body(i):
            r = pl.multiple_of(i * 256, 256)
            part[2, pl.ds(r, 256), lanes(SUMS[2][g])] = (
                last_last(gcot[pl.ds(r, 256)], w_all[0, pl.ds(128 * first, 128 * n)])
                + last_last(ucot[pl.ds(r, 256)], w_all[1, pl.ds(128 * first, 128 * n)])
            ).astype(BF)

        tiles(2, body)
        pass_sum(2, g, 0, part, 256, 256, pair, 0, partner)

    @scoped
    def cotangent():
        values = mixed[0].astype(F32)
        inverse = lax.rsqrt(jnp.mean(values * values, axis=-1, keepdims=True) + NORM_EPS)
        scaled = inverse**3 * jnp.mean(weighted[...] * values, axis=-1, keepdims=True)
        for g in (3, 2, 1, 0):
            at = slice(512 * g, 512 * g + 512)
            cot[0:64, at] = (
                inverse * weighted[:, at] - mixed[0, :, at].astype(F32) * scaled
            ).astype(BF)

    @scoped
    def hidden(g):
        def body(i):
            r = pl.multiple_of(i * 256, 256)
            term = jnp.dot(
                cot[pl.ds(r, 256), pl.ds(512 * g, 512)],
                w_all[2, pl.ds(512 * g, 512)],
                preferred_element_type=F32,
            )
            hcot[pl.ds(r, 256)] = hcot[pl.ds(r, 256)] + term if begun else term

        tiles(2, body)
        begun.append(g)

    @scoped
    def dgrad(g):
        first, n = BLOCKS[g]
        grads[2, pl.ds(128 * first, 128 * n)] = first_first(
            cot[:, lanes(BLOCKS[g])], hid[1]
        ).astype(BF)

    @scoped
    def turn():
        for k in range(16):
            tok_t[128 * k : 128 * k + 128] = tok[1, :, 128 * k : 128 * k + 128].T

    @scoped
    def derive():
        gcot[...] = (hcot[...] * dgate[...]).astype(BF)
        ucot[...] = (hcot[...] * dup[...]).astype(BF)

    @scoped
    def wgrad(w, g):
        def body(i):
            r = pl.multiple_of(512 * g + i * 256, 256)
            grads[w, pl.ds(r, 256)] = jnp.dot(
                tok_t[pl.ds(r, 256)], (gcot, ucot)[w][...], preferred_element_type=F32
            ).astype(BF)

        tiles(2, body)

    @scoped
    def late_end():
        values = mixed[1].astype(F32)
        inverse = lax.rsqrt(jnp.mean(values * values, axis=-1, keepdims=True) + NORM_EPS)
        for k, at in enumerate(columns):
            late_out[:, pl.ds(at, 128)] = (
                late_v[:, pl.ds(at, 128)].astype(F32)
                + 0.5
                * mixed[1, :, 128 * k : 128 * k + 128].astype(F32)
                * inverse
                * post_v[:, pl.ds(at, 128)]
            ).astype(BF)

    @scoped
    def early_end():
        early = early_v[...].astype(F32)
        inverse = lax.rsqrt(jnp.mean(early * early, axis=-1, keepdims=True) + NORM_EPS)
        dots = jnp.zeros((64, 128), F32)
        for k, at in enumerate(columns):
            dots += (
                mixed[2, :, 128 * k : 128 * k + 128].astype(F32)
                * pre_v[:, pl.ds(at, 128)]
                * early_v[:, pl.ds(at, 128)].astype(F32)
            )
        slope = inverse**3 * (jnp.sum(dots, axis=-1, keepdims=True) * (1.0 / 2048.0))
        for k, at in enumerate(columns):
            early_out[:, pl.ds(at, 128)] = (
                grad_v[:, pl.ds(at, 128)].astype(F32)
                + inverse
                * (mixed[2, :, 128 * k : 128 * k + 128].astype(F32) * pre_v[:, pl.ds(at, 128)])
                - early_v[:, pl.ds(at, 128)].astype(F32) * slope
            ).astype(BF)

    begun = []
    steps = (
        own, relay, norm, spread, near, far, full, weigh, gate, up, down, back, start, middle,
        summed, turn, cotangent, hidden, dgrad, derive, wgrad, combine, late_end, early_end,
        pass_on, give,
    )
    for name, *at in SCRIPT:
        steps[name](*at)

    def leave(ref, ss):
        pltpu.make_async_remote_copy(
            src_ref=ref, dst_ref=ref, send_sem=ss, recv_sem=ss,
            device_id=partner, device_id_type=MESH,
        ).wait_send()

    leave(w_all.reshape(3 * 2048, 512).at[pl.ds(0, 3 * 15 * 128)], ag_s)
    leave(grads.reshape(3 * 2048, 512).at[pl.ds(0, 3 * 15 * 128)], rs_s)
    leave(tok.reshape(1024, 2048).at[pl.ds(0, 2 * 448)], xa_s.at[0])
    leave(cot.at[pl.ds(0, 448)], xa_s.at[1])
    leave(part.reshape(3 * 512, 2048).at[pl.ds(0, 3 * 448)], xr_s)


def hand_over(*refs):
    copies = [pltpu.make_async_copy(refs[i], refs[5 + i], refs[10].at[i]) for i in range(5)]
    for copy in copies:
        copy.start()
    for copy in copies:
        copy.wait()


def per_device(
    late_input,
    early_input,
    early_grad,
    pre_gain,
    post_gain,
    gate_weight,
    up_weight,
    down_weight,
    gate_sum,
    up_sum,
    down_gradient_sum,
):
    sem = pltpu.SemaphoreType.DMA
    vmem = pltpu.VMEM
    tokens = jax.ShapeDtypeStruct((64, 2048), BF)
    total = jax.ShapeDtypeStruct((128, 512), F32)
    results = pl.pallas_call(
        kernel,
        name="half_step",
        out_shape=(vmem((64, 2048), BF),) * 2 + (vmem((128, 512), F32),) * 3,
        in_specs=[pl.BlockSpec(memory_space=pl.ANY)] * 11,
        out_specs=[pl.BlockSpec(memory_space=vmem)] * 5,
        scratch_shapes=[
            vmem((64, 2048), BF),
            vmem((64, 2048), BF),
            vmem((64, 2048), BF),
            vmem((1, 2048), F32),
            vmem((1, 2048), F32),
            vmem((128, 512), F32),
            vmem((128, 512), F32),
            vmem((128, 512), F32),
            vmem((3, 2048, 512), BF),
            vmem((2, 512, 2048), BF),
            vmem((2048, 512), BF),
            vmem((2, 512, 512), F32),
            vmem((512, 512), F32),
            vmem((512, 512), F32),
            vmem((2, 512, 512), BF),
            vmem((3, 512, 2048), BF),
            vmem((3, 256, 2048), BF),
            vmem((3, 256, 2048), BF),
            vmem((3, 64, 2048), BF),
            vmem((3, 192, 2048), BF),
            vmem((512, 2048), BF),
            vmem((512, 512), F32),
            vmem((512, 512), BF),
            vmem((512, 512), BF),
            vmem((3, 2048, 512), BF),
            vmem((3 * PIECES, ARRIVED_ROWS, 512), BF),
            vmem((3, 64, 2048), BF),
            vmem((64, 2048), F32),
            sem,
            sem((3 * PIECES, 15)),
            sem,
            sem((3 * PIECES, len(GAINS))),
            sem((2,)),
            sem((2 + len(BLOCKS), 4)),
            sem,
            sem((SUM_AT[2] + len(SUMS[2]), 4)),
            sem((11,)),
        ],
        compiler_params=pltpu.CompilerParams(
            collective_id=0, has_side_effects=True, vmem_limit_bytes=60 * 2**20
        ),
    )(
        late_input, early_input, early_grad, pre_gain.reshape(1, -1), post_gain.reshape(1, -1),
        gate_weight, up_weight, down_weight, gate_sum, up_sum, down_gradient_sum,
    )
    return pl.pallas_call(
        hand_over,
        name="hand_over",
        out_shape=(tokens, tokens, total, total, total),
        in_specs=[pl.BlockSpec(memory_space=vmem)] * 5,
        out_specs=[pl.BlockSpec(memory_space=pl.ANY)] * 5,
        scratch_shapes=[sem((5,))],
        compiler_params=pltpu.CompilerParams(vmem_limit_bytes=4 * 2**20),
    )(*results)


def solution(mesh):
    rows, both = P(("fs", "tp"), None), P("fs", "tp")
    return jax.shard_map(
        per_device,
        mesh=mesh,
        in_specs=(rows,) * 3 + (P(), P()) + (both,) * 6,
        out_specs=(rows, rows, both, both, both),
        check_vma=False,
    )
```
